256 devices in a mesh: grp: 2 (over y), ep: 32 (over z, core), tp: 4 (over x).
Axes of the slice: x: 4, y: 2, z: 16, core: 2. Of those that a mesh axis runs over, the one named last changes fastest.
The devices are a block of a 4x16x16 slice.
Arguments:
- hidden_in: bfloat16 [32768, 2048], P(('grp', 'ep', 'tp')), parts along dimension 0, may hold values from -6 to 6
- expert_ids: int32 [32768, 2], P(('grp', 'ep', 'tp')), parts along dimension 0, may hold values from 0 to 127, all different within a row; in each aligned block of 128 rows (0 to 127, 128 to 255, ...) at most 4 rows name the same one
- route_weights: float32 [32768, 2], P(('grp', 'ep', 'tp')), parts along dimension 0, may hold values from 0.1 to 1
- norm_gain: float32 [2048], replicated, may hold values from 0.1 to 1.9
- gate_proj: bfloat16 [128, 2048, 512], P(('ep', 'tp')), may hold values from -0.125 to 0.125
- up_proj: bfloat16 [128, 2048, 512], P(('ep', 'tp')), may hold values from -0.125 to 0.125
- down_proj: bfloat16 [128, 512, 2048], P(('ep', 'tp')), may hold values from -0.25 to 0.25
Outputs:
- mixed_out: bfloat16 [32768, 2048], P(('grp', 'ep', 'tp')), parts along dimension 0
The draws below stay inside these ranges and needn't reach their ends.
There are 2 independent parts, one for each index of `grp`. The reference program is written for one: setup_inputs(seed, part) draws one part's arguments, and reference() takes and returns one part's arrays. A program takes and returns all parts, laid end to end along the dimension named above; an argument that names none is the same for every part. Nothing has to cross between parts.
Inputs may be any that keep to these rules, and one draw needn't show every extreme that they name: `expert_ids`: each token names 2 different experts; among the 128 tokens of one device (aligned blocks of rows) no expert is named more than 4 times, and in every draw some expert is named exactly 4 times by some device's tokens.
All inputs are finite; a program needn't handle non-finite values.
Results may differ from the reference program's by a relative error of at most 0.0071.
Values may be sent and summed in bfloat16 or wider, within the bound.
A program may use at most 64 MiB of HBM per device.

```python
import math
import jax
import jax.numpy as jnp
import numpy as np
from jax import lax

D = 2048
FE = 512
TOP_K = 2
TOK_DEV = 128
EXPERTS = 128
TOKENS = 16384
CAP = 4
N_EP = 32
N_TP = 4


def block_levels(stream_key, shape, cuts, least, high):
    gain, own = 1.0, jax.random.fold_in(stream_key, 6)
    for dim, blocks in cuts:
        steps = jnp.exp(jax.random.uniform(jax.random.fold_in(own, dim), (blocks,), jnp.float32, least / len(cuts), high / len(cuts)))
        gain = gain * jnp.repeat(steps, shape[dim] // blocks).reshape([-1 if axis == dim else 1 for axis in range(len(shape))])
    return gain


def shared_out(key, own, number, rows, amount, top, reach, lean):
    ranking = jax.random.permutation(key, amount)
    packed, ordinary = portions_of(amount, rows * top, reach, lean, True), portions_of(amount, rows * top, reach, lean, False)
    places = jnp.arange(amount)

    def named(lengths, offset_by):
        used = int((lengths > 0).sum())
        fixed = max(1, used // 4)
        passed = fixed + (places - fixed + offset_by * (used - fixed)) % max(1, amount - fixed)
        return jnp.zeros((amount,), jnp.int32).at[ranking[jnp.where(places < fixed, places, passed)]].set(jnp.asarray(lengths, jnp.int32))

    lengths = jnp.where(number % 4 == 0, named(packed, number // 4), named(ordinary, number - number // 4 - 1))
    mixed = jax.random.permutation(jax.random.fold_in(own, 3), amount)
    donor, taker = mixed[0:amount // 2 * 2:2], mixed[1:amount // 2 * 2:2]
    room = jnp.minimum(lengths[donor] - 1, reach - lengths[taker]) // 2
    room = jnp.where((donor == ranking[0]) | (taker == ranking[0]) | (lengths[taker] == 0), 0, jnp.maximum(room, 0))
    passed = jax.random.randint(jax.random.fold_in(own, 4), (amount // 2,), 0, 1 << 20) % (room + 1)
    lengths = lengths.at[donor].add(-passed).at[taker].add(passed)
    labels = jnp.searchsorted(jnp.cumsum(lengths), jnp.arange(rows * top), side="right").astype(jnp.int32)
    listing = labels.reshape(top, rows).T
    listing = listing[jax.random.permutation(jax.random.fold_in(own, 1), rows)]
    offset_by = jax.random.randint(jax.random.fold_in(own, 2), (rows, 1), 0, top)
    return jnp.take_along_axis(listing, (jnp.arange(top)[None, :] + offset_by) % top, axis=1)


def portions_of(amount, total, most, lean, full):
    weights = [(1 << 20) // math.isqrt(rank ** lean) + 1 for rank in range(1, amount + 1)]
    largest = most if full else min(most, max(-(-total // amount), total * weights[0] // sum(weights)))
    least = 1 if total - largest >= amount - 1 else 0
    given, surplus = [largest] + [least] * (amount - 1), total - largest - least * (amount - 1)
    while surplus > 0:
        free = [i for i in range(1, amount) if given[i] < largest] or [i for i in range(1, amount) if given[i] < most]
        mass, remaining = sum([weights[i] for i in free]), surplus
        for i in free:
            addition = min(most - given[i], max(1, remaining * weights[i] // mass), surplus)
            given[i] = given[i] + addition
            surplus = surplus - addition
    return np.array(given)


def gaussian(stream_key, extent, deviation, most, split=(), held_as=jnp.bfloat16):
    result = jax.random.normal(stream_key, extent, jnp.float32) * deviation
    if len(split) > 0:
        result = block_levels(stream_key, extent, split, -0.22, 0.18) * result
    return jnp.clip(result, min=-most, max=most).astype(held_as)


def setup_inputs(seed: int = 0, part: int = 0) -> dict:
    splits = jax.random.split(jax.random.key(seed), 8)
    own_keys = jax.random.split(jax.random.fold_in(splits[7], part), 8)
    hidden_in = gaussian(own_keys[0], (TOKENS, D), 1.0, 6.0, ((0, 128),))
    expert_ids_keys = jax.random.split(jax.random.fold_in(own_keys[1], 1), TOKENS // TOK_DEV)
    expert_ids_turns = jax.random.permutation(jax.random.fold_in(own_keys[1], 3), TOKENS // TOK_DEV)
    expert_ids = jax.vmap(lambda own, number: shared_out(jax.random.fold_in(own_keys[1], 2), own, number, TOK_DEV, EXPERTS, TOP_K, CAP, 2))(expert_ids_keys, expert_ids_turns).reshape((TOKENS, TOP_K))
    route_weights = jnp.clip(jnp.exp(math.log(1.0) - 2.3025851 * jax.random.uniform(own_keys[2], (TOKENS, TOP_K), jnp.float32) ** block_levels(own_keys[2], (TOKENS, TOP_K), ((0, 128),), -0.2, 0.2)), 0.1, 1.0)
    norm_gain = jnp.clip(1.0 + 0.18 * jax.random.normal(splits[3], (D,), jnp.float32), 0.1, 1.9)
    gate_proj = gaussian(splits[4], (EXPERTS, D, FE), D ** -0.5, 0.125, ((0, 128),))
    up_proj = gaussian(splits[5], (EXPERTS, D, FE), D ** -0.5, 0.125, ((0, 128),))
    down_proj = gaussian(splits[6], (EXPERTS, FE, D), FE ** -0.5, 0.25, ((0, 128),))
    return dict(hidden_in=hidden_in, expert_ids=expert_ids, route_weights=route_weights, norm_gain=norm_gain, gate_proj=gate_proj, up_proj=up_proj, down_proj=down_proj)


def reference(hidden_in, expert_ids, route_weights, norm_gain, gate_proj, up_proj, down_proj):
    device_count = N_EP * N_TP
    as_float = hidden_in.astype(jnp.float32)
    scaled = as_float * lax.rsqrt(lax.optimization_barrier(jnp.mean(as_float * as_float, axis=-1, keepdims=True)) + 1e-06)
    normed = (scaled * norm_gain).astype(jnp.bfloat16)
    flat_ids = expert_ids.reshape(device_count, TOK_DEV * TOP_K).astype(jnp.int32)
    onehot = (flat_ids[:, :, None] == jnp.arange(EXPERTS, dtype=jnp.int32)[None, None, :]).astype(jnp.int32)
    slot_index = lax.optimization_barrier(jnp.sum((jnp.cumsum(onehot, axis=1) - onehot) * onehot, axis=2)).astype(jnp.int32)
    source = jnp.arange(device_count, dtype=jnp.int32)[:, None]
    target = (flat_ids * (device_count * CAP) + source * CAP + slot_index).reshape(-1).astype(jnp.int32)
    routed = jnp.repeat(normed, TOP_K, axis=0)
    expert_rows = jnp.zeros((EXPERTS * device_count * CAP, D), jnp.bfloat16).at[target].set(routed)
    expert_rows = expert_rows.reshape(EXPERTS, device_count * CAP, D)

    def run_expert(pieces):
        block_in, weight_gate, weight_up, weight_down = pieces
        block_float = block_in.astype(jnp.float32)
        gate_act = jnp.dot(block_float, weight_gate.astype(jnp.float32))
        up_act = jnp.dot(block_float, weight_up.astype(jnp.float32))
        hidden = (jax.nn.silu(gate_act) * up_act).astype(jnp.bfloat16)
        return jnp.dot(hidden.astype(jnp.float32), weight_down.astype(jnp.float32)).astype(jnp.bfloat16)
    expert_out = lax.map(run_expert, (expert_rows, gate_proj, up_proj, down_proj))
    picked = expert_out.reshape(-1, D)[target].astype(jnp.float32).reshape(TOKENS, TOP_K, D)
    return lax.optimization_barrier(jnp.sum(picked * route_weights[:, :, None], axis=1)).astype(jnp.bfloat16)
```

```python
import functools

import jax
import jax.numpy as jnp
from jax import lax
from jax.experimental import pallas as pl
from jax.experimental.pallas import tpu as pltpu
from jax.sharding import PartitionSpec as P

MESH = pl.DeviceIdType.MESH
BF = jnp.bfloat16
F32 = jnp.float32
I32 = jnp.int32
Q = 4


def mm(a, b):
    return jnp.dot(a, b, preferred_element_type=F32)


def mm_nt(a, b):
    return lax.dot_general(a, b, (((1,), (1,)), ((), ())), preferred_element_type=F32)


class Dims:
    def __init__(self, ep, tp, tokens, width, fe, cap):
        self.NZ, self.NX = ep // 2, tp
        self.T, self.D, self.FE, self.CAP = tokens, width, fe, cap
        self.DQ = width // Q
        self.H = self.NZ // 2
        self.PL = 2 * tp
        self.RB = Q * cap
        self.NR = self.PL * self.RB
        self.HB = self.H // 2
        self.SR = self.PL * 2 * cap
        plane = self.PL * cap
        self.caps = [tokens] + [
            min(tokens, (self.H - k) * plane + plane // 2) for k in range(1, self.H + 1)
        ]
        packed = [k for k in range(1, self.H + 1) if self.caps[k] < tokens]
        self.KP = packed[0] if packed else self.H + 1


def kernel(
    dm, hid, meta, gain, wg, wu, wd, out,
    xs, metas, zb, zp, rin, rout, stage, rows, ysend, yrecv,
    ex, cm, sm, st, erow, upper, perm_g, perm_s, acc, xb, gacc, uacc, hb, yb,
    wgv, wuv, wdv,
    w_sem, m_send, m_recv, z_send, z_recv, p_send, p_recv, y_send, y_recv, r_send, r_recv,
):
    NZ, NX, T, D, FE, CAP = dm.NZ, dm.NX, dm.T, dm.D, dm.FE, dm.CAP
    DQ, H, PL, RB, NR, HB, SR, KP, caps = dm.DQ, dm.H, dm.PL, dm.RB, dm.NR, dm.HB, dm.SR, dm.KP, dm.caps
    ep, x = lax.axis_index("ep"), lax.axis_index("tp")
    z, c = ep // 2, ep % 2

    def at_z(other):
        return {"ep": other * 2 + c, "tp": x}

    def in_plane(j):
        dc, dx = j // NX, j % NX
        return {"ep": z * 2 + (c + dc) % 2, "tp": (x + dx) % NX}

    def mirror(j):
        return (j // NX) * NX + (NX - j % NX) % NX

    barrier = pltpu.get_barrier_semaphore()
    for d in range(1, NZ):
        pl.semaphore_signal(barrier, inc=1, device_id=at_z((z + d) % NZ), device_id_type=MESH)
    for j in range(1, PL):
        pl.semaphore_signal(barrier, inc=1, device_id=in_plane(j), device_id_type=MESH)

    weight_copies = []
    for q in range(Q):
        weight_copies.append(pltpu.make_async_copy(wg.at[0, pl.ds(q * DQ, DQ)], wgv.at[q], w_sem.at[0, q]))
        weight_copies.append(pltpu.make_async_copy(wu.at[0, pl.ds(q * DQ, DQ)], wuv.at[q], w_sem.at[1, q]))
        weight_copies.append(pltpu.make_async_copy(wd.at[0, :, pl.ds(q * DQ, DQ)], wdv.at[q], w_sem.at[2, q]))
    for copy in weight_copies:
        copy.start()

    NB = 16

    def norm_rows(b, _):
        r = pl.ds(pl.multiple_of(b * NB, NB), NB)
        v = hid[r, :].astype(F32)
        scale = lax.rsqrt(jnp.mean(v * v, axis=-1, keepdims=True) + 1e-06)
        n = ((v * scale) * gain[...]).astype(BF)
        for q in range(Q):
            xs[q, r, :] = n[:, q * DQ:(q + 1) * DQ]
        return 0

    lax.fori_loop(0, T // NB, norm_rows, 0)

    metas[0] = meta[...]
    r_id = lax.broadcasted_iota(I32, (NR, T), 0)
    j_id = r_id // RB
    dx_id, dc_id = j_id % NX, j_id // NX
    erow[...] = z * PL + ((c + dc_id) % 2) * NX + (x + dx_id) % NX
    slot_row = lax.broadcasted_iota(I32, (NR, T), 0) % CAP
    t_row = lax.broadcasted_iota(I32, (T, T), 0)
    t_col = lax.broadcasted_iota(I32, (T, T), 1)
    upper[...] = jnp.where(t_row < t_col, 1.0, 0.0).astype(BF)
    PR = Q * SR
    a_id = lax.broadcasted_iota(I32, (PR, PR), 0)
    n_id = lax.broadcasted_iota(I32, (PR, PR), 1)
    q_of, m_of = a_id // SR, a_id % SR
    perm_g[...] = jnp.where(n_id == (m_of // CAP) * RB + q_of * CAP + m_of % CAP, 1.0, 0.0).astype(BF)
    q_of, m_of = n_id // SR, n_id % SR
    perm_s[...] = jnp.where(a_id == (m_of // CAP) * RB + q_of * CAP + m_of % CAP, 1.0, 0.0).astype(BF)

    pl.semaphore_wait(barrier, NZ - 1 + PL - 1)

    meta_copies = [
        pltpu.make_async_remote_copy(
            src_ref=meta, dst_ref=metas.at[d], send_sem=m_send.at[d], recv_sem=m_recv.at[d],
            device_id=at_z((z + d) % NZ), device_id_type=MESH,
        )
        for d in range(1, NZ)
    ]
    for copy in meta_copies:
        copy.start()

    def z_copy(src, direction, k, q, rows_sent):
        return pltpu.make_async_remote_copy(
            src_ref=src, dst_ref=zb.at[direction, k - 1, q, pl.ds(0, rows_sent)],
            send_sem=z_send.at[direction, k - 1, q], recv_sem=z_recv.at[direction, k - 1, q],
            device_id=at_z((z + 1 - 2 * direction + NZ) % NZ), device_id_type=MESH,
        )

    def send_own(i, _):
        q, direction = i // 2, i % 2
        z_copy(xs.at[q], direction, 1, q, caps[1]).start()
        return 0

    lax.fori_loop(0, 2 * Q, send_own, 0)

    def build(direction, k):
        d = k + direction * (NZ - 2 * k)
        s = (z - d + NZ) % NZ
        m = metas[d]
        ids = [m[i:i + 1, :].astype(I32) for i in range(2)]
        wts = [m[2 + i:3 + i, :] for i in range(2)]
        e = erow[...]
        hit0, hit1 = e == ids[0], e == ids[1]
        hit = jnp.where(hit0, 1.0, 0.0) + jnp.where(hit1, 1.0, 0.0)
        count = mm(hit.astype(BF), upper[...])
        last = jnp.where(k == H, 1, 0)
        other_way = last * jnp.where(e % 2 == direction, 0, 1)
        sel = jnp.where(count == slot_row.astype(F32), hit, 0.0)
        sel = jnp.where(other_way == 1, 0.0, sel)
        pick = sel.astype(BF)
        weighted = ((jnp.where(hit0, wts[0], 0.0) + jnp.where(hit1, wts[1], 0.0)) * sel).astype(BF)

        reach = jnp.zeros((1, T), I32)
        for i in range(2):
            dist = ids[i] // PL - s
            dist = jnp.where(dist < 0, dist + NZ, dist)
            odd = ids[i] % 2
            up_way = jnp.where(dist < H, dist, jnp.where((dist == H) & (odd == 0), H, 0))
            down_way = jnp.where(dist > H, NZ - dist, jnp.where((dist == H) & (odd == 1), H, 0))
            reach = jnp.maximum(reach, jnp.where(direction == 0, up_way, down_way))

        def place(kk):
            mask = jnp.where(reach >= kk, 1.0, 0.0)
            pos = mm(jnp.broadcast_to(mask, (8, T)).astype(BF), upper[...])[0:1, :].astype(I32)
            pos = jnp.where(reach >= kk, pos, -1)
            col = lax.broadcasted_iota(I32, (1, T), 1)
            pos = jnp.where(kk >= KP, pos, col)
            return jnp.where(t_row == pos, 1.0, 0.0).astype(BF)

        here, after = place(k), place(k + 1)
        ex[direction, k] = mm_nt(pick, here).astype(BF)
        cm[direction, k] = mm_nt(here, weighted).astype(BF)
        sm[direction, k] = mm_nt(after, here).astype(BF)
        st[direction, k] = mm_nt(here, after).astype(BF)

    def build_steps(lo, hi):
        def one(i, _):
            build(i % 2, lo + i // 2)
            return 0

        lax.fori_loop(0, 2 * (hi - lo), one, 0)

    q_row = (lax.broadcasted_iota(I32, (NR, 1), 0) // CAP) % Q

    def only_q_rows(v, q):
        return jnp.where(q_row == q, v.astype(F32), 0.0).astype(BF)

    q_col = (lax.broadcasted_iota(I32, (1, NR), 1) // CAP) % Q

    def only_q_cols(v, q):
        return jnp.where(q_col == q, v.astype(F32), 0.0).astype(BF)

    build(0, 0)
    own = jnp.zeros((NR, DQ), F32)
    for q in range(Q):
        own = own + mm(only_q_rows(ex[0, 0], q), xs[q])
    own = own.astype(BF).reshape(PL, RB, DQ)
    stage[H - 1, :, 1] = own
    rows[H - 1, 0, 1] = own[0]

    for copy in meta_copies:
        copy.wait()

    def dispatch(k):
        ck = caps[k]
        acc[...] = jnp.zeros_like(acc)

        def chunk(i, _):
            q, direction = i // 2, i % 2
            z_copy(zb.at[direction, k - 1, q, pl.ds(0, ck)], direction, k, q, ck).wait_recv()
            data = zb[direction, k - 1, q, pl.ds(0, ck), :]
            if k < H:
                cn = caps[k + 1]
                if k + 1 >= KP:
                    p = k + 1 - KP
                    zp[direction, p, q, pl.ds(0, cn), :] = mm(
                        sm[direction, k, pl.ds(0, cn), pl.ds(0, ck)] if ck == T else sm[direction, k][:cn, :ck], data
                    ).astype(BF)
                    source = zp.at[direction, p, q, pl.ds(0, cn)]
                else:
                    source = zb.at[direction, k - 1, q, pl.ds(0, cn)]
                z_copy(source, direction, k + 1, q, cn).start()
            e = only_q_rows(ex[direction, k], q)
            if ck < T:
                e = e[:, :ck]
            block = direction if k < H else 0
            acc[block] = acc[block] + mm(e, data)
            return 0

        lax.fori_loop(0, 2 * Q, chunk, 0)
        for block in range(2 if k < H else 1):
            v = acc[block].astype(BF).reshape(PL, RB, DQ)
            stage[k - 1, :, block] = v
            rows[k - 1, 0, block] = v[0]
        for j in range(1, PL):
            plane_copy(stage, rows, k, j, p_send, p_recv).start()

    def plane_copy(src, dst, k, j, send, recv):
        return pltpu.make_async_remote_copy(
            src_ref=src.at[k - 1, j], dst_ref=dst.at[k - 1, mirror(j)],
            send_sem=send.at[k - 1, j], recv_sem=recv.at[k - 1, mirror(j)],
            device_id=in_plane(j), device_id_type=MESH,
        )

    def plane_wait(src, dst, k, send, recv):
        for j in range(1, PL):
            plane_copy(src, dst, k, mirror(j), send, recv).wait_recv()

    def experts(k0):
        BR = HB * SR
        for i in range(HB):
            k = k0 + i
            plane_wait(stage, rows, k, p_send, p_recv)
            got = mm(perm_g[...], rows[k - 1].reshape(PR, DQ)).astype(BF).reshape(Q, SR, DQ)
            xb[:, pl.ds(i * SR, SR), :] = got
        gacc[...] = jnp.zeros_like(gacc)
        uacc[...] = jnp.zeros_like(uacc)

        def inner(q, _):
            v = xb[q]
            gacc[...] += mm(v, wgv[q])
            uacc[...] += mm(v, wuv[q])
            return 0

        lax.fori_loop(0, Q, inner, 0)
        g = gacc[...]
        hb[...] = ((g / (1.0 + jnp.exp(-g))) * uacc[...]).astype(BF)

        def outer(q, _):
            yb[q] = mm(hb[...], wdv[q]).astype(BF)
            return 0

        lax.fori_loop(0, Q, outer, 0)
        for i in range(HB):
            k = k0 + i
            v = yb[:, pl.ds(i * SR, SR), :].reshape(PR, DQ)
            v = mm(perm_s[...], v).astype(BF).reshape(PL, 2, RB, DQ)
            ysend[k - 1] = v
            yrecv[k - 1, 0] = v[0]
            for j in range(1, PL):
                plane_copy(ysend, yrecv, k, j, y_send, y_recv).start()

    build_steps(1, min(3, H + 1))
    built = min(3, H + 1)
    for k in range(1, H + 1):
        dispatch(k)
        if built <= H:
            nxt = min(built + 2, H + 1)
            build_steps(built, nxt)
            built = nxt
        if k == 1:
            for copy in weight_copies:
                copy.wait()
        if k == HB + 1:
            experts(1)
    experts(HB + 1)

    def r_copy(direction, k, q):
        return pltpu.make_async_remote_copy(
            src_ref=rout.at[direction, k - 1, q, pl.ds(0, caps[k])],
            dst_ref=rin.at[direction, k - 1, q, pl.ds(0, caps[k])],
            send_sem=r_send.at[direction, k - 1, q], recv_sem=r_recv.at[direction, k - 1, q],
            device_id=at_z((z - 1 + 2 * direction + NZ) % NZ), device_id_type=MESH,
        )

    for k in range(H, 0, -1):
        ck = caps[k]
        plane_wait(ysend, yrecv, k, y_send, y_recv)

        def back(i, _, k=k, ck=ck):
            q, direction = i // 2, i % 2
            block = direction if k < H else 0
            y = yrecv[k - 1, :, block].reshape(NR, DQ)
            v = mm(only_q_cols(cm[direction, k, pl.ds(0, ck), :], q), y)
            if k < H:
                cn = caps[k + 1]
                r_copy(direction, k + 1, q).wait_recv()
                far = rin[direction, k, q, pl.ds(0, cn), :]
                if k + 1 >= KP:
                    v = v + mm(st[direction, k][:ck, :cn], far)
                else:
                    v = v + far.astype(F32)
            rout[direction, k - 1, q, pl.ds(0, ck), :] = v.astype(BF)
            r_copy(direction, k, q).start()
            return 0

        lax.fori_loop(0, 2 * Q, back, 0)

    y_own = yrecv[H - 1, :, 1].reshape(NR, DQ)
    for q in range(Q):
        v = mm(only_q_cols(cm[0, 0], q), y_own)
        for direction in range(2):
            r_copy(direction, 1, q).wait_recv()
            v = v + rin[direction, 0, q].astype(F32)
        out[:, q * DQ:(q + 1) * DQ] = v.astype(BF)

    for k in range(1, H + 1):
        def drained(i, _, k=k):
            q, direction = i // 2, i % 2
            z_copy(xs.at[q, pl.ds(0, caps[k])], direction, k, q, caps[k]).wait_send()
            r_copy(direction, k, q).wait_send()
            return 0

        lax.fori_loop(0, 2 * Q, drained, 0)
        for j in range(1, PL):
            plane_copy(stage, rows, k, j, p_send, p_recv).wait_send()
            plane_copy(ysend, yrecv, k, j, y_send, y_recv).wait_send()


def body(hidden_in, expert_ids, route_weights, norm_gain, gate_proj, up_proj, down_proj):
    tokens, width = hidden_in.shape
    chosen = expert_ids.shape[1]
    ep, tp = lax.axis_size("ep"), lax.axis_size("tp")
    fe = gate_proj.shape[2]
    cap = max(2, 2 * chosen * tokens // (ep * tp))
    dm = Dims(ep, tp, tokens, width, fe, cap)
    meta = jnp.concatenate(
        [expert_ids.T.astype(F32), route_weights.T, jnp.zeros((4, tokens), F32)], axis=0
    )
    H, T, DQ, PL, RB, NR, NZ, SR, HB = dm.H, dm.T, dm.DQ, dm.PL, dm.RB, dm.NR, dm.NZ, dm.SR, dm.HB
    vm = pltpu.VMEM
    packed = max(1, H - dm.KP + 1)
    dma = pltpu.SemaphoreType.DMA
    return pl.pallas_call(
        functools.partial(kernel, dm),
        out_shape=jax.ShapeDtypeStruct((tokens, width), BF),
        in_specs=[pl.BlockSpec(memory_space=vm)] * 3 + [pl.BlockSpec(memory_space=pl.ANY)] * 3,
        out_specs=pl.BlockSpec(memory_space=vm),
        scratch_shapes=[
            vm((Q, T, DQ), BF),
            vm((NZ, 8, T), F32),
            vm((2, H, Q, T, DQ), BF),
            vm((2, packed, Q, dm.caps[min(dm.KP, H)], DQ), BF),
            vm((2, H, Q, T, DQ), BF),
            vm((2, H, Q, T, DQ), BF),
            vm((H, PL, 2, RB, DQ), BF),
            vm((H, PL, 2, RB, DQ), BF),
            vm((H, PL, 2, RB, DQ), BF),
            vm((H, PL, 2, RB, DQ), BF),
            vm((2, H + 1, NR, T), BF),
            vm((2, H + 1, T, NR), BF),
            vm((2, H + 1, T, T), BF),
            vm((2, H + 1, T, T), BF),
            vm((NR, T), I32),
            vm((T, T), BF),
            vm((Q * SR, Q * SR), BF),
            vm((Q * SR, Q * SR), BF),
            vm((2, NR, DQ), F32),
            vm((Q, HB * SR, DQ), BF),
            vm((HB * SR, fe), F32),
            vm((HB * SR, fe), F32),
            vm((HB * SR, fe), BF),
            vm((Q, HB * SR, DQ), BF),
            vm((Q, DQ, fe), BF),
            vm((Q, DQ, fe), BF),
            vm((Q, fe, DQ), BF),
            dma((3, Q)),
            dma((NZ,)),
            dma((NZ,)),
            dma((2, H, Q)),
            dma((2, H, Q)),
            dma((H, PL)),
            dma((H, PL)),
            dma((H, PL)),
            dma((H, PL)),
            dma((2, H, Q)),
            dma((2, H, Q)),
        ],
        compiler_params=pltpu.CompilerParams(
            collective_id=0, has_side_effects=True, vmem_limit_bytes=66 * 1000 * 1000
        ),
        name="routed_experts",
    )(hidden_in, meta, norm_gain.reshape(1, width), gate_proj, up_proj, down_proj)


def solution(mesh):
    return jax.shard_map(
        body,
        mesh=mesh,
        in_specs=(
            P(("grp", "ep", "tp"), None),
            P(("grp", "ep", "tp"), None),
            P(("grp", "ep", "tp"), None),
            P(),
            P(("ep", "tp"), None, None),
            P(("ep", "tp"), None, None),
            P(("ep", "tp"), None, None),
        ),
        out_specs=P(("grp", "ep", "tp"), None),
        check_vma=False,
    )
```

```python
import functools

import jax
import jax.numpy as jnp
from jax import lax
from jax.experimental import pallas as pl
from jax.experimental.pallas import tpu as pltpu
from jax.sharding import PartitionSpec as P

MESH = pl.DeviceIdType.MESH
BF = jnp.bfloat16
F32 = jnp.float32
I32 = jnp.int32
Q = 4


def mm(a, b):
    return jnp.dot(a, b, preferred_element_type=F32)


def mm_nt(a, b):
    return lax.dot_general(a, b, (((1,), (1,)), ((), ())), preferred_element_type=F32)


class Dims:
    def __init__(self, ep, tp, tokens, width, fe, cap):
        self.NZ, self.NX = ep // 2, tp
        self.T, self.D, self.FE, self.CAP = tokens, width, fe, cap
        self.DQ = width // Q
        self.H = self.NZ // 2
        self.PL = 2 * tp
        self.RB = Q * cap
        self.NR = self.PL * self.RB
        self.SR = self.PL * 2 * cap
        plane = self.PL * cap
        self.caps = [tokens] + [
            min(tokens, (self.H - k) * plane + plane // 2) for k in range(1, self.H + 1)
        ]
        packed = [k for k in range(1, self.H + 1) if self.caps[k] < tokens]
        self.KP = packed[0] if packed else self.H + 1


def kernel(
    dm, hid, ids_in, wts_in, gain, wg, wu, wd, out,
    xs, metas, zb, zp, rin, rout, stage, rows, ysend, yrecv,
    ex, cm, sm, st, erow, upper, perm_g, perm_s, acc, xb, gacc, uacc, hb, yb,
    wgv, wuv, wdv,
    w_sem, m_send, m_recv, z_send, z_recv, p_send, p_recv, y_send, y_recv, r_send, r_recv,
):
    NZ, NX, T, D, FE, CAP = dm.NZ, dm.NX, dm.T, dm.D, dm.FE, dm.CAP
    DQ, H, PL, RB, NR, SR, KP, caps = dm.DQ, dm.H, dm.PL, dm.RB, dm.NR, dm.SR, dm.KP, dm.caps
    ep, x = lax.axis_index("ep"), lax.axis_index("tp")
    z, c = ep // 2, ep % 2

    def at_z(other):
        return {"ep": other * 2 + c, "tp": x}

    def onward(direction):
        return at_z((z + 1 - 2 * direction + NZ) % NZ)

    def backward(direction):
        return at_z((z - 1 + 2 * direction + NZ) % NZ)

    def in_plane(j):
        dc, dx = j // NX, j % NX
        return {"ep": z * 2 + (c + dc) % 2, "tp": (x + dx) % NX}

    def mirror(j):
        return (j // NX) * NX + (NX - j % NX) % NX

    barrier = pltpu.get_barrier_semaphore()
    for direction in range(2):
        pl.semaphore_signal(barrier, inc=1, device_id=onward(direction), device_id_type=MESH)
    for j in range(1, PL):
        pl.semaphore_signal(barrier, inc=1, device_id=in_plane(j), device_id_type=MESH)

    weight_copies = []
    for q in range(Q):
        weight_copies.append(pltpu.make_async_copy(wg.at[0, pl.ds(q * DQ, DQ)], wgv.at[q], w_sem.at[0, q]))
        weight_copies.append(pltpu.make_async_copy(wu.at[0, pl.ds(q * DQ, DQ)], wuv.at[q], w_sem.at[1, q]))
        weight_copies.append(pltpu.make_async_copy(wd.at[0, :, pl.ds(q * DQ, DQ)], wdv.at[q], w_sem.at[2, q]))
    for copy in weight_copies:
        copy.start()

    NB = 16

    def norm_rows(b, _):
        r = pl.ds(pl.multiple_of(b * NB, NB), NB)
        v = hid[r, :].astype(F32)
        scale = lax.rsqrt(jnp.mean(v * v, axis=-1, keepdims=True) + 1e-06)
        n = ((v * scale) * gain[...]).astype(BF)
        for q in range(Q):
            xs[q, r, :] = n[:, q * DQ:(q + 1) * DQ]
        return 0

    lax.fori_loop(0, T // NB, norm_rows, 0)

    for direction in range(2):
        metas[direction, 0, 0:2, :] = ids_in[...].astype(F32)
        metas[direction, 0, 2:4, :] = wts_in[...]
    r_id = lax.broadcasted_iota(I32, (NR, T), 0)
    j_id = r_id // RB
    dx_id, dc_id = j_id % NX, j_id // NX
    erow[...] = z * PL + ((c + dc_id) % 2) * NX + (x + dx_id) % NX
    slot_row = lax.broadcasted_iota(I32, (NR, T), 0) % CAP
    t_row = lax.broadcasted_iota(I32, (T, T), 0)
    t_col = lax.broadcasted_iota(I32, (T, T), 1)
    upper[...] = jnp.where(t_row < t_col, 1.0, 0.0).astype(BF)
    PR = Q * SR
    a_id = lax.broadcasted_iota(I32, (PR, PR), 0)
    n_id = lax.broadcasted_iota(I32, (PR, PR), 1)
    q_of, m_of = a_id // SR, a_id % SR
    perm_g[...] = jnp.where(n_id == (m_of // CAP) * RB + q_of * CAP + m_of % CAP, 1.0, 0.0).astype(BF)
    q_of, m_of = n_id // SR, n_id % SR
    perm_s[...] = jnp.where(a_id == (m_of // CAP) * RB + q_of * CAP + m_of % CAP, 1.0, 0.0).astype(BF)

    def z_copy(src, direction, k, q, rows_sent):
        return pltpu.make_async_remote_copy(
            src_ref=src, dst_ref=zb.at[direction, k - 1, q, pl.ds(0, rows_sent)],
            send_sem=z_send.at[direction, k - 1, q], recv_sem=z_recv.at[direction, k - 1, q],
            device_id=onward(direction), device_id_type=MESH,
        )

    def m_copy(direction, k):
        return pltpu.make_async_remote_copy(
            src_ref=metas.at[direction, k - 1], dst_ref=metas.at[direction, k],
            send_sem=m_send.at[direction, k], recv_sem=m_recv.at[direction, k],
            device_id=onward(direction), device_id_type=MESH,
        )

    def relay_meta(direction, k):
        m_copy(direction, k).wait_recv()

        @pl.when(k < H)
        def _():
            m_copy(direction, k + 1).start()

    def plane_copy(src, dst, t, j, send, recv):
        if t < H:
            here, there = src.at[t - 1, j], dst.at[t - 1, mirror(j)]
        else:
            here, there = src.at[H - 1, j, t - H], dst.at[H - 1, mirror(j), t - H]
        return pltpu.make_async_remote_copy(
            src_ref=here, dst_ref=there, send_sem=send.at[t - 1, j], recv_sem=recv.at[t - 1, mirror(j)],
            device_id=in_plane(j), device_id_type=MESH,
        )

    def plane_start(src, dst, t, send, recv):
        for j in range(1, PL):
            plane_copy(src, dst, t, j, send, recv).start()

    def plane_wait(src, dst, t, send, recv):
        for j in range(1, PL):
            plane_copy(src, dst, t, mirror(j), send, recv).wait_recv()

    def plane_sent(src, dst, t, send, recv):
        for j in range(1, PL):
            plane_copy(src, dst, t, j, send, recv).wait_send()

    def build(direction, k):
        s = (z + NZ - k + 2 * k * direction) % NZ
        m = metas[direction, k]
        ids = [m[i:i + 1, :].astype(I32) for i in range(2)]
        wts = [m[2 + i:3 + i, :] for i in range(2)]
        e = erow[...]
        hit0, hit1 = e == ids[0], e == ids[1]
        hit = jnp.where(hit0, 1.0, 0.0) + jnp.where(hit1, 1.0, 0.0)
        count = mm(hit.astype(BF), upper[...])
        last = jnp.where(k == H, 1, 0)
        other_way = last * jnp.where(e % 2 == direction, 0, 1)
        sel = jnp.where(count == slot_row.astype(F32), hit, 0.0)
        sel = jnp.where(other_way == 1, 0.0, sel)
        pick = sel.astype(BF)
        weighted = ((jnp.where(hit0, wts[0], 0.0) + jnp.where(hit1, wts[1], 0.0)) * sel).astype(BF)

        reach = jnp.zeros((1, T), I32)
        for i in range(2):
            dist = ids[i] // PL - s
            dist = jnp.where(dist < 0, dist + NZ, dist)
            odd = ids[i] % 2
            up_way = jnp.where(dist < H, dist, jnp.where((dist == H) & (odd == 0), H, 0))
            down_way = jnp.where(dist > H, NZ - dist, jnp.where((dist == H) & (odd == 1), H, 0))
            reach = jnp.maximum(reach, jnp.where(direction == 0, up_way, down_way))

        def place(kk):
            mask = jnp.where(reach >= kk, 1.0, 0.0)
            pos = mm(jnp.broadcast_to(mask, (8, T)).astype(BF), upper[...])[0:1, :].astype(I32)
            pos = jnp.where(reach >= kk, pos, -1)
            col = lax.broadcasted_iota(I32, (1, T), 1)
            pos = jnp.where(kk >= KP, pos, col)
            return jnp.where(t_row == pos, 1.0, 0.0).astype(BF)

        here, after = place(k), place(k + 1)
        ex[direction, k] = mm_nt(pick, here).astype(BF)
        cm[direction, k] = mm_nt(here, weighted).astype(BF)
        sm[direction, k] = mm_nt(after, here).astype(BF)
        st[direction, k] = mm_nt(here, after).astype(BF)

    def build_steps(lo, hi):
        def one(i, _):
            build(i % 2, lo + i // 2)
            return 0

        lax.fori_loop(0, 2 * (hi - lo), one, 0)

    q_row = (lax.broadcasted_iota(I32, (NR, 1), 0) // CAP) % Q

    def only_q_rows(v, q):
        return jnp.where(q_row == q, v.astype(F32), 0.0).astype(BF)

    q_col = (lax.broadcasted_iota(I32, (1, NR), 1) // CAP) % Q

    def only_q_cols(v, q):
        return jnp.where(q_col == q, v.astype(F32), 0.0).astype(BF)

    def own_block():
        build(0, 0)
        acc[0] = jnp.zeros((NR, DQ), F32)

        def one(q, _):
            acc[0] = acc[0] + mm(only_q_rows(ex[0, 0], q), xs[q])
            return 0

        lax.fori_loop(0, Q, one, 0)
        own = acc[0].astype(BF).reshape(PL, RB, DQ)
        stage[H - 1, :, 1] = own
        rows[H - 1, 0, 1] = own[0]
        plane_start(stage, rows, H + 1, p_send, p_recv)

    def gather(k0):
        for i in range(2):
            k = k0 + i
            plane_wait(stage, rows, k, p_send, p_recv)
            if k == H:
                plane_wait(stage, rows, H + 1, p_send, p_recv)
            got = mm(perm_g[...], rows[k - 1].reshape(PR, DQ)).astype(BF).reshape(Q, SR, DQ)
            xb[:, pl.ds(i * SR, SR), :] = got
        gacc[...] = jnp.zeros_like(gacc)
        uacc[...] = jnp.zeros_like(uacc)

    def piece(i):
        @pl.when(i < Q)
        def _():
            gacc[...] += mm(xb[i], wgv[i])
            uacc[...] += mm(xb[i], wuv[i])

        @pl.when(i == Q)
        def _():
            g = gacc[...]
            hb[...] = ((g / (1.0 + jnp.exp(-g))) * uacc[...]).astype(BF)

        @pl.when(i >= Q)
        def _():
            yb[i - Q] = mm(hb[...], wdv[i - Q]).astype(BF)

    def scatter(k0):
        for i in range(2):
            k = k0 + i
            v = yb[:, pl.ds(i * SR, SR), :].reshape(PR, DQ)
            v = mm(perm_s[...], v).astype(BF).reshape(PL, 2, RB, DQ)
            ysend[k - 1] = v
            yrecv[k - 1, 0] = v[0]

    def experts(k0):
        gather(k0)

        def one(i, _):
            piece(i)
            return 0

        lax.fori_loop(0, 2 * Q, one, 0)
        scatter(k0)

    def dispatch(k, beside):
        ck = caps[k]
        acc[...] = jnp.zeros_like(acc)

        def chunk(i, _):
            q, direction = i // 2, i % 2
            z_copy(zb.at[direction, k - 1, q, pl.ds(0, ck)], direction, k, q, ck).wait_recv()
            data = zb[direction, k - 1, q, pl.ds(0, ck), :]
            if k < H:
                cn = caps[k + 1]
                if k + 1 >= KP:
                    p = k + 1 - KP
                    zp[direction, p, q, pl.ds(0, cn), :] = mm(sm[direction, k][:cn, :ck], data).astype(BF)
                    source = zp.at[direction, p, q, pl.ds(0, cn)]
                else:
                    source = zb.at[direction, k - 1, q, pl.ds(0, cn)]
                z_copy(source, direction, k + 1, q, cn).start()
            if k == 1:
                @pl.when(q + Q <= H)
                def _():
                    relay_meta(direction, q + Q)
            e = only_q_rows(ex[direction, k], q)
            if ck < T:
                e = e[:, :ck]
            block = direction if k < H else 0
            acc[block] = acc[block] + mm(e, data)
            if beside:
                piece(i)
            return 0

        lax.fori_loop(0, 2 * Q, chunk, 0)
        for block in range(2 if k < H else 1):
            v = acc[block].astype(BF).reshape(PL, RB, DQ)
            stage[k - 1, :, block] = v
            rows[k - 1, 0, block] = v[0]
        plane_start(stage, rows, k, p_send, p_recv)

    firsts = list(range(1, H, 2))
    beside = {k0 + 3: k0 for k0 in firsts if k0 + 3 <= H - 2}
    after = [k0 for k0 in firsts if k0 + 3 > H - 2]

    pl.semaphore_wait(barrier, 2 + PL - 1)
    for direction in range(2):
        m_copy(direction, 1).start()
    for q in range(Q):
        for direction in range(2):
            z_copy(xs.at[q], direction, 1, q, caps[1]).start()
        if q == 0:
            own_block()
        if 1 <= q + 1 < Q and q + 1 <= H:
            for direction in range(2):
                relay_meta(direction, q + 1)
        if q == 0:
            build_steps(1, 2)

    dispatch(1, False)
    for k in range(2 * Q, H + 1):
        for direction in range(2):
            relay_meta(direction, k)
    for copy in weight_copies:
        copy.wait()
    built = 2
    for k in range(1, H + 1):
        if k > 1:
            if k in beside:
                gather(beside[k])
            dispatch(k, k in beside)
            if k in beside:
                scatter(beside[k])
                for i in range(2):
                    plane_start(ysend, yrecv, beside[k] + i, y_send, y_recv)
        nxt = min(built + 2, H + 1)
        if built < nxt:
            build_steps(built, nxt)
        built = nxt
    for k0 in after:
        experts(k0)
    for k in range(H, after[0] - 1, -1):
        plane_start(ysend, yrecv, k, y_send, y_recv)
    plane_start(ysend, yrecv, H + 1, y_send, y_recv)

    def r_copy(direction, k, q):
        return pltpu.make_async_remote_copy(
            src_ref=rout.at[direction, k - 1, q, pl.ds(0, caps[k])],
            dst_ref=rin.at[direction, k - 1, q, pl.ds(0, caps[k])],
            send_sem=r_send.at[direction, k - 1, q], recv_sem=r_recv.at[direction, k - 1, q],
            device_id=backward(direction), device_id_type=MESH,
        )

    for k in range(H, 0, -1):
        ck = caps[k]
        plane_wait(ysend, yrecv, k, y_send, y_recv)

        def back(i, _, k=k, ck=ck):
            q, direction = i // 2, i % 2
            block = direction if k < H else 0
            y = yrecv[k - 1, :, block].reshape(NR, DQ)
            v = mm(only_q_cols(cm[direction, k, pl.ds(0, ck), :], q), y)
            if k < H:
                cn = caps[k + 1]
                r_copy(direction, k + 1, q).wait_recv()
                far = rin[direction, k, q, pl.ds(0, cn), :]
                if k + 1 >= KP:
                    v = v + mm(st[direction, k][:ck, :cn], far)
                else:
                    v = v + far.astype(F32)
            rout[direction, k - 1, q, pl.ds(0, ck), :] = v.astype(BF)
            r_copy(direction, k, q).start()
            z_copy(xs.at[q, pl.ds(0, ck)], direction, k, q, ck).wait_send()
            if k < H:
                r_copy(direction, k + 1, q).wait_send()
            return 0

        lax.fori_loop(0, 2 * Q, back, 0)
        plane_sent(stage, rows, k, p_send, p_recv)
        plane_sent(ysend, yrecv, k, y_send, y_recv)
        for direction in range(2):
            m_copy(direction, k).wait_send()

    plane_sent(stage, rows, H + 1, p_send, p_recv)
    plane_sent(ysend, yrecv, H + 1, y_send, y_recv)
    plane_wait(ysend, yrecv, H + 1, y_send, y_recv)
    y_own = yrecv[H - 1, :, 1].reshape(NR, DQ)
    for q in range(Q):
        v = mm(only_q_cols(cm[0, 0], q), y_own)
        for direction in range(2):
            r_copy(direction, 1, q).wait_recv()
            v = v + rin[direction, 0, q].astype(F32)
        out[:, q * DQ:(q + 1) * DQ] = v.astype(BF)
    for q in range(Q):
        for direction in range(2):
            r_copy(direction, 1, q).wait_send()


def body(hidden_in, expert_ids, route_weights, norm_gain, gate_proj, up_proj, down_proj):
    tokens, width = hidden_in.shape
    chosen = expert_ids.shape[1]
    ep, tp = lax.axis_size("ep"), lax.axis_size("tp")
    fe = gate_proj.shape[2]
    cap = max(2, 2 * chosen * tokens // (ep * tp))
    dm = Dims(ep, tp, tokens, width, fe, cap)
    H, T, DQ, PL, RB, NR, SR = dm.H, dm.T, dm.DQ, dm.PL, dm.RB, dm.NR, dm.SR
    vm = pltpu.VMEM
    packed = max(1, H - dm.KP + 1)
    dma = pltpu.SemaphoreType.DMA
    return pl.pallas_call(
        functools.partial(kernel, dm),
        out_shape=jax.ShapeDtypeStruct((tokens, width), BF),
        in_specs=[pl.BlockSpec(memory_space=vm)] * 4 + [pl.BlockSpec(memory_space=pl.ANY)] * 3,
        out_specs=pl.BlockSpec(memory_space=vm),
        scratch_shapes=[
            vm((Q, T, DQ), BF),
            vm((2, H + 1, 4, T), F32),
            vm((2, H, Q, T, DQ), BF),
            vm((2, packed, Q, dm.caps[min(dm.KP, H)], DQ), BF),
            vm((2, H, Q, T, DQ), BF),
            vm((2, H, Q, T, DQ), BF),
            vm((H, PL, 2, RB, DQ), BF),
            vm((H, PL, 2, RB, DQ), BF),
            vm((H, PL, 2, RB, DQ), BF),
            vm((H, PL, 2, RB, DQ), BF),
            vm((2, H + 1, NR, T), BF),
            vm((2, H + 1, T, NR), BF),
            vm((2, H + 1, T, T), BF),
            vm((2, H + 1, T, T), BF),
            vm((NR, T), I32),
            vm((T, T), BF),
            vm((Q * SR, Q * SR), BF),
            vm((Q * SR, Q * SR), BF),
            vm((2, NR, DQ), F32),
            vm((Q, 2 * SR, DQ), BF),
            vm((2 * SR, fe), F32),
            vm((2 * SR, fe), F32),
            vm((2 * SR, fe), BF),
            vm((Q, 2 * SR, DQ), BF),
            vm((Q, DQ, fe), BF),
            vm((Q, DQ, fe), BF),
            vm((Q, fe, DQ), BF),
            dma((3, Q)),
            dma((2, H + 1)),
            dma((2, H + 1)),
            dma((2, H, Q)),
            dma((2, H, Q)),
            dma((H + 1, PL)),
            dma((H + 1, PL)),
            dma((H + 1, PL)),
            dma((H + 1, PL)),
            dma((2, H, Q)),
            dma((2, H, Q)),
        ],
        compiler_params=pltpu.CompilerParams(
            collective_id=0, has_side_effects=True, vmem_limit_bytes=66 * 1000 * 1000
        ),
        name="routed_experts",
    )(hidden_in, expert_ids.T, route_weights.T, norm_gain.reshape(1, width), gate_proj, up_proj, down_proj)


def solution(mesh):
    return jax.shard_map(
        body,
        mesh=mesh,
        in_specs=(
            P(("grp", "ep", "tp"), None),
            P(("grp", "ep", "tp"), None),
            P(("grp", "ep", "tp"), None),
            P(),
            P(("ep", "tp"), None, None),
            P(("ep", "tp"), None, None),
            P(("ep", "tp"), None, None),
        ),
        out_specs=P(("grp", "ep", "tp"), None),
        check_vma=False,
    )
```

```python
import functools

import jax
import jax.numpy as jnp
from jax import lax
from jax.experimental import pallas as pl
from jax.experimental.pallas import tpu as pltpu
from jax.sharding import PartitionSpec as P

MESH = pl.DeviceIdType.MESH
BF = jnp.bfloat16
F32 = jnp.float32
I32 = jnp.int32
Q = 4


def mm(a, b):
    return jnp.dot(a, b, preferred_element_type=F32)


def mm_nt(a, b):
    return lax.dot_general(a, b, (((1,), (1,)), ((), ())), preferred_element_type=F32)


class Dims:
    def __init__(self, ep, tp, tokens, width, fe, cap):
        self.NZ, self.NX = ep // 2, tp
        self.T, self.D, self.FE, self.CAP = tokens, width, fe, cap
        self.DQ = width // Q
        self.H = self.NZ // 2
        self.PL = 2 * tp
        self.RB = Q * cap
        self.NR = self.PL * self.RB
        self.SR = self.PL * 2 * cap
        plane = self.PL * cap
        self.caps = [tokens] + [
            min(tokens, (self.H - k) * plane + plane // 2) for k in range(1, self.H + 1)
        ]
        packed = [k for k in range(1, self.H + 1) if self.caps[k] < tokens]
        self.KP = packed[0] if packed else self.H + 1


def kernel(
    dm, hid, ids_in, wts_in, gain, wg, wu, wd, out,
    xs, metas, zb, zp, rin, rout, stage, rows, ysend, yrecv,
    ex, cm, sm, st, erow, upper, perm_g, perm_s, acc, xb, gacc, uacc, hb, yb,
    wgv, wuv, wdv,
    w_sem, m_send, m_recv, z_send, z_recv, p_send, p_recv, y_send, y_recv, r_send, r_recv,
):
    NZ, NX, T, D, FE, CAP = dm.NZ, dm.NX, dm.T, dm.D, dm.FE, dm.CAP
    DQ, H, PL, RB, NR, SR, KP, caps = dm.DQ, dm.H, dm.PL, dm.RB, dm.NR, dm.SR, dm.KP, dm.caps
    ep, x = lax.axis_index("ep"), lax.axis_index("tp")
    z, c = ep // 2, ep % 2

    def at_z(other):
        return {"ep": other * 2 + c, "tp": x}

    def onward(direction):
        return at_z((z + 1 - 2 * direction + NZ) % NZ)

    def backward(direction):
        return at_z((z - 1 + 2 * direction + NZ) % NZ)

    def in_plane(j):
        dc, dx = j // NX, j % NX
        return {"ep": z * 2 + (c + dc) % 2, "tp": (x + dx) % NX}

    def mirror(j):
        return (j // NX) * NX + (NX - j % NX) % NX

    barrier = pltpu.get_barrier_semaphore()
    for direction in range(2):
        pl.semaphore_signal(barrier, inc=1, device_id=onward(direction), device_id_type=MESH)
    for j in range(1, PL):
        pl.semaphore_signal(barrier, inc=1, device_id=in_plane(j), device_id_type=MESH)

    weight_copies = []
    for q in range(Q):
        weight_copies.append(pltpu.make_async_copy(wg.at[0, pl.ds(q * DQ, DQ)], wgv.at[q], w_sem.at[0, q]))
        weight_copies.append(pltpu.make_async_copy(wu.at[0, pl.ds(q * DQ, DQ)], wuv.at[q], w_sem.at[1, q]))
        weight_copies.append(pltpu.make_async_copy(wd.at[0, :, pl.ds(q * DQ, DQ)], wdv.at[q], w_sem.at[2, q]))
    for copy in weight_copies:
        copy.start()

    NB = 16

    def norm_rows(b, _):
        r = pl.ds(pl.multiple_of(b * NB, NB), NB)
        v = hid[r, :].astype(F32)
        scale = lax.rsqrt(jnp.mean(v * v, axis=-1, keepdims=True) + 1e-06)
        n = ((v * scale) * gain[...]).astype(BF)
        for q in range(Q):
            xs[q, r, :] = n[:, q * DQ:(q + 1) * DQ]
        return 0

    lax.fori_loop(0, T // NB, norm_rows, 0)

    for direction in range(2):
        metas[direction, 0, 0:2, :] = ids_in[...].astype(F32)
        metas[direction, 0, 2:4, :] = wts_in[...]
    r_id = lax.broadcasted_iota(I32, (NR, T), 0)
    j_id = r_id // RB
    dx_id, dc_id = j_id % NX, j_id // NX
    erow[...] = z * PL + ((c + dc_id) % 2) * NX + (x + dx_id) % NX
    slot_row = lax.broadcasted_iota(I32, (NR, T), 0) % CAP
    t_row = lax.broadcasted_iota(I32, (T, T), 0)
    t_col = lax.broadcasted_iota(I32, (T, T), 1)
    upper[...] = jnp.where(t_row < t_col, 1.0, 0.0).astype(BF)
    PR = Q * SR
    a_id = lax.broadcasted_iota(I32, (PR, PR), 0)
    n_id = lax.broadcasted_iota(I32, (PR, PR), 1)
    q_of, m_of = a_id // SR, a_id % SR
    perm_g[...] = jnp.where(n_id == (m_of // CAP) * RB + q_of * CAP + m_of % CAP, 1.0, 0.0).astype(BF)
    q_of, m_of = n_id // SR, n_id % SR
    perm_s[...] = jnp.where(a_id == (m_of // CAP) * RB + q_of * CAP + m_of % CAP, 1.0, 0.0).astype(BF)

    def z_copy(src, direction, k, q, rows_sent):
        return pltpu.make_async_remote_copy(
            src_ref=src, dst_ref=zb.at[direction, k - 1, q, pl.ds(0, rows_sent)],
            send_sem=z_send.at[direction, k - 1, q], recv_sem=z_recv.at[direction, k - 1, q],
            device_id=onward(direction), device_id_type=MESH,
        )

    def m_copy(direction, k):
        return pltpu.make_async_remote_copy(
            src_ref=metas.at[direction, k - 1], dst_ref=metas.at[direction, k],
            send_sem=m_send.at[direction, k], recv_sem=m_recv.at[direction, k],
            device_id=onward(direction), device_id_type=MESH,
        )

    def relay_meta(direction, k):
        m_copy(direction, k).wait_recv()

        @pl.when(k < H)
        def _():
            m_copy(direction, k + 1).start()

    def plane_copy(src, dst, t, j, send, recv):
        if t < H:
            here, there = src.at[t - 1, j], dst.at[t - 1, mirror(j)]
        else:
            here, there = src.at[H - 1, j, t - H], dst.at[H - 1, mirror(j), t - H]
        return pltpu.make_async_remote_copy(
            src_ref=here, dst_ref=there, send_sem=send.at[t - 1, j], recv_sem=recv.at[t - 1, mirror(j)],
            device_id=in_plane(j), device_id_type=MESH,
        )

    def plane_start(src, dst, t, send, recv):
        for j in range(1, PL):
            plane_copy(src, dst, t, j, send, recv).start()

    def plane_wait(src, dst, t, send, recv):
        for j in range(1, PL):
            plane_copy(src, dst, t, mirror(j), send, recv).wait_recv()

    def plane_sent(src, dst, t, send, recv):
        for j in range(1, PL):
            plane_copy(src, dst, t, j, send, recv).wait_send()

    def build(direction, k):
        s = (z + NZ - k + 2 * k * direction) % NZ
        m = metas[direction, k]
        ids = [m[i:i + 1, :].astype(I32) for i in range(2)]
        wts = [m[2 + i:3 + i, :] for i in range(2)]
        e = erow[...]
        hit0, hit1 = e == ids[0], e == ids[1]
        hit = jnp.where(hit0, 1.0, 0.0) + jnp.where(hit1, 1.0, 0.0)
        count = mm(hit.astype(BF), upper[...])
        last = jnp.where(k == H, 1, 0)
        other_way = last * jnp.where(e % 2 == direction, 0, 1)
        sel = jnp.where(count == slot_row.astype(F32), hit, 0.0)
        sel = jnp.where(other_way == 1, 0.0, sel)
        pick = sel.astype(BF)
        weighted = ((jnp.where(hit0, wts[0], 0.0) + jnp.where(hit1, wts[1], 0.0)) * sel).astype(BF)

        reach = jnp.zeros((1, T), I32)
        for i in range(2):
            dist = ids[i] // PL - s
            dist = jnp.where(dist < 0, dist + NZ, dist)
            odd = ids[i] % 2
            up_way = jnp.where(dist < H, dist, jnp.where((dist == H) & (odd == 0), H, 0))
            down_way = jnp.where(dist > H, NZ - dist, jnp.where((dist == H) & (odd == 1), H, 0))
            reach = jnp.maximum(reach, jnp.where(direction == 0, up_way, down_way))

        def place(kk):
            mask = jnp.where(reach >= kk, 1.0, 0.0)
            pos = mm(jnp.broadcast_to(mask, (8, T)).astype(BF), upper[...])[0:1, :].astype(I32)
            pos = jnp.where(reach >= kk, pos, -1)
            col = lax.broadcasted_iota(I32, (1, T), 1)
            pos = jnp.where(kk >= KP, pos, col)
            return jnp.where(t_row == pos, 1.0, 0.0).astype(BF)

        here, after = place(k), place(k + 1)
        ex[direction, k] = mm_nt(pick, here).astype(BF)
        cm[direction, k] = mm_nt(here, weighted).astype(BF)
        sm[direction, k] = mm_nt(after, here).astype(BF)
        st[direction, k] = mm_nt(here, after).astype(BF)

    def build_steps(lo, hi):
        def one(i, _):
            build(i % 2, lo + i // 2)
            return 0

        lax.fori_loop(0, 2 * (hi - lo), one, 0)

    q_row = (lax.broadcasted_iota(I32, (NR, 1), 0) // CAP) % Q

    def only_q_rows(v, q):
        return jnp.where(q_row == q, v.astype(F32), 0.0).astype(BF)

    q_col = (lax.broadcasted_iota(I32, (1, NR), 1) // CAP) % Q

    def only_q_cols(v, q):
        return jnp.where(q_col == q, v.astype(F32), 0.0).astype(BF)

    def own_block():
        build(0, 0)
        acc[0] = jnp.zeros((NR, DQ), F32)

        def one(q, _):
            acc[0] = acc[0] + mm(only_q_rows(ex[0, 0], q), xs[q])
            return 0

        lax.fori_loop(0, Q, one, 0)
        own = acc[0].astype(BF).reshape(PL, RB, DQ)
        stage[H - 1, :, 1] = own
        rows[H - 1, 0, 1] = own[0]
        plane_start(stage, rows, H + 1, p_send, p_recv)

    def gather(k0):
        for i in range(2):
            k = k0 + i
            plane_wait(stage, rows, k, p_send, p_recv)
            if k == H:
                plane_wait(stage, rows, H + 1, p_send, p_recv)
            got = mm(perm_g[...], rows[k - 1].reshape(PR, DQ)).astype(BF).reshape(Q, SR, DQ)
            xb[:, pl.ds(i * SR, SR), :] = got
        gacc[...] = jnp.zeros_like(gacc)
        uacc[...] = jnp.zeros_like(uacc)

    def piece(i):
        @pl.when(i < Q)
        def _():
            gacc[...] += mm(xb[i], wgv[i])
            uacc[...] += mm(xb[i], wuv[i])

        @pl.when(i == Q)
        def _():
            g = gacc[...]
            hb[...] = ((g / (1.0 + jnp.exp(-g))) * uacc[...]).astype(BF)

        @pl.when(i >= Q)
        def _():
            yb[i - Q] = mm(hb[...], wdv[i - Q]).astype(BF)

    def scatter(k0):
        for i in range(2):
            k = k0 + i
            v = yb[:, pl.ds(i * SR, SR), :].reshape(PR, DQ)
            v = mm(perm_s[...], v).astype(BF).reshape(PL, 2, RB, DQ)
            ysend[k - 1] = v
            yrecv[k - 1, 0] = v[0]

    def experts(k0):
        gather(k0)

        def one(i, _):
            piece(i)
            return 0

        lax.fori_loop(0, 2 * Q, one, 0)
        scatter(k0)

    def dispatch(k, beside):
        ck = caps[k]
        acc[...] = jnp.zeros_like(acc)

        def chunk(i, _):
            q, direction = i // 2, i % 2
            base = Q - 1 + 2 * (k - 1)
            if base <= H:
                @pl.when((q % 2 == 1) & (base + q // 2 <= H))
                def _():
                    relay_meta(direction, base + q // 2)
            z_copy(zb.at[direction, k - 1, q, pl.ds(0, ck)], direction, k, q, ck).wait_recv()
            data = zb[direction, k - 1, q, pl.ds(0, ck), :]
            if k < H:
                cn = caps[k + 1]
                if k + 1 >= KP:
                    p = k + 1 - KP
                    zp[direction, p, q, pl.ds(0, cn), :] = mm(sm[direction, k][:cn, :ck], data).astype(BF)
                    source = zp.at[direction, p, q, pl.ds(0, cn)]
                else:
                    source = zb.at[direction, k - 1, q, pl.ds(0, cn)]
                z_copy(source, direction, k + 1, q, cn).start()
            e = only_q_rows(ex[direction, k], q)
            if ck < T:
                e = e[:, :ck]
            block = direction if k < H else 0
            acc[block] = acc[block] + mm(e, data)
            if beside:
                piece(i)
            return 0

        lax.fori_loop(0, 2 * Q, chunk, 0)
        for block in range(2 if k < H else 1):
            v = acc[block].astype(BF).reshape(PL, RB, DQ)
            stage[k - 1, :, block] = v
            rows[k - 1, 0, block] = v[0]
        plane_start(stage, rows, k, p_send, p_recv)

    firsts = list(range(1, H, 2))
    beside = {k0 + 3: k0 for k0 in firsts if k0 + 3 <= H - 2}
    after = [k0 for k0 in firsts if k0 + 3 > H - 2]

    pl.semaphore_wait(barrier, 2 + PL - 1)
    for direction in range(2):
        m_copy(direction, 1).start()
    for q in range(2):
        for direction in range(2):
            z_copy(xs.at[q], direction, 1, q, caps[1]).start()
    own_block()
    for q in range(2, Q):
        for direction in range(2):
            relay_meta(direction, q - 1)
        for direction in range(2):
            z_copy(xs.at[q], direction, 1, q, caps[1]).start()
        if q == 2:
            build_steps(1, 2)

    dispatch(1, False)
    for copy in weight_copies:
        copy.wait()
    built = 2
    for k in range(1, H + 1):
        if k > 1:
            if k in beside:
                gather(beside[k])
            dispatch(k, k in beside)
            if k in beside:
                scatter(beside[k])
                for i in range(2):
                    plane_start(ysend, yrecv, beside[k] + i, y_send, y_recv)
        nxt = min(built + 2, H + 1)
        if built < nxt:
            build_steps(built, nxt)
        built = nxt
    for k0 in after:
        experts(k0)
    for k in range(H, after[0] - 1, -1):
        plane_start(ysend, yrecv, k, y_send, y_recv)
    plane_start(ysend, yrecv, H + 1, y_send, y_recv)

    def r_copy(direction, k, q):
        return pltpu.make_async_remote_copy(
            src_ref=rout.at[direction, k - 1, q, pl.ds(0, caps[k])],
            dst_ref=rin.at[direction, k - 1, q, pl.ds(0, caps[k])],
            send_sem=r_send.at[direction, k - 1, q], recv_sem=r_recv.at[direction, k - 1, q],
            device_id=backward(direction), device_id_type=MESH,
        )

    for k in range(H, 0, -1):
        ck = caps[k]
        plane_wait(ysend, yrecv, k, y_send, y_recv)

        def back(i, _, k=k, ck=ck):
            q, direction = i // 2, i % 2
            block = direction if k < H else 0
            y = yrecv[k - 1, :, block].reshape(NR, DQ)
            v = mm(only_q_cols(cm[direction, k, pl.ds(0, ck), :], q), y)
            if k < H:
                cn = caps[k + 1]
                r_copy(direction, k + 1, q).wait_recv()
                far = rin[direction, k, q, pl.ds(0, cn), :]
                if k + 1 >= KP:
                    v = v + mm(st[direction, k][:ck, :cn], far)
                else:
                    v = v + far.astype(F32)
            rout[direction, k - 1, q, pl.ds(0, ck), :] = v.astype(BF)
            r_copy(direction, k, q).start()
            z_copy(xs.at[q, pl.ds(0, ck)], direction, k, q, ck).wait_send()
            if k < H:
                r_copy(direction, k + 1, q).wait_send()
            return 0

        lax.fori_loop(0, 2 * Q, back, 0)
        plane_sent(stage, rows, k, p_send, p_recv)
        plane_sent(ysend, yrecv, k, y_send, y_recv)
        for direction in range(2):
            m_copy(direction, k).wait_send()

    plane_sent(stage, rows, H + 1, p_send, p_recv)
    plane_sent(ysend, yrecv, H + 1, y_send, y_recv)
    plane_wait(ysend, yrecv, H + 1, y_send, y_recv)
    y_own = yrecv[H - 1, :, 1].reshape(NR, DQ)
    for q in range(Q):
        v = mm(only_q_cols(cm[0, 0], q), y_own)
        for direction in range(2):
            r_copy(direction, 1, q).wait_recv()
            v = v + rin[direction, 0, q].astype(F32)
        out[:, q * DQ:(q + 1) * DQ] = v.astype(BF)
    for q in range(Q):
        for direction in range(2):
            r_copy(direction, 1, q).wait_send()


def body(hidden_in, expert_ids, route_weights, norm_gain, gate_proj, up_proj, down_proj):
    tokens, width = hidden_in.shape
    chosen = expert_ids.shape[1]
    ep, tp = lax.axis_size("ep"), lax.axis_size("tp")
    fe = gate_proj.shape[2]
    cap = max(2, 2 * chosen * tokens // (ep * tp))
    dm = Dims(ep, tp, tokens, width, fe, cap)
    H, T, DQ, PL, RB, NR, SR = dm.H, dm.T, dm.DQ, dm.PL, dm.RB, dm.NR, dm.SR
    vm = pltpu.VMEM
    packed = max(1, H - dm.KP + 1)
    dma = pltpu.SemaphoreType.DMA
    return pl.pallas_call(
        functools.partial(kernel, dm),
        out_shape=jax.ShapeDtypeStruct((tokens, width), BF),
        in_specs=[pl.BlockSpec(memory_space=vm)] * 4 + [pl.BlockSpec(memory_space=pl.ANY)] * 3,
        out_specs=pl.BlockSpec(memory_space=vm),
        scratch_shapes=[
            vm((Q, T, DQ), BF),
            vm((2, H + 1, 4, T), F32),
            vm((2, H, Q, T, DQ), BF),
            vm((2, packed, Q, dm.caps[min(dm.KP, H)], DQ), BF),
            vm((2, H, Q, T, DQ), BF),
            vm((2, H, Q, T, DQ), BF),
            vm((H, PL, 2, RB, DQ), BF),
            vm((H, PL, 2, RB, DQ), BF),
            vm((H, PL, 2, RB, DQ), BF),
            vm((H, PL, 2, RB, DQ), BF),
            vm((2, H + 1, NR, T), BF),
            vm((2, H + 1, T, NR), BF),
            vm((2, H + 1, T, T), BF),
            vm((2, H + 1, T, T), BF),
            vm((NR, T), I32),
            vm((T, T), BF),
            vm((Q * SR, Q * SR), BF),
            vm((Q * SR, Q * SR), BF),
            vm((2, NR, DQ), F32),
            vm((Q, 2 * SR, DQ), BF),
            vm((2 * SR, fe), F32),
            vm((2 * SR, fe), F32),
            vm((2 * SR, fe), BF),
            vm((Q, 2 * SR, DQ), BF),
            vm((Q, DQ, fe), BF),
            vm((Q, DQ, fe), BF),
            vm((Q, fe, DQ), BF),
            dma((3, Q)),
            dma((2, H + 1)),
            dma((2, H + 1)),
            dma((2, H, Q)),
            dma((2, H, Q)),
            dma((H + 1, PL)),
            dma((H + 1, PL)),
            dma((H + 1, PL)),
            dma((H + 1, PL)),
            dma((2, H, Q)),
            dma((2, H, Q)),
        ],
        compiler_params=pltpu.CompilerParams(
            collective_id=0, has_side_effects=True, vmem_limit_bytes=66 * 1000 * 1000
        ),
        name="routed_experts",
    )(hidden_in, expert_ids.T, route_weights.T, norm_gain.reshape(1, width), gate_proj, up_proj, down_proj)


def solution(mesh):
    return jax.shard_map(
        body,
        mesh=mesh,
        in_specs=(
            P(("grp", "ep", "tp"), None),
            P(("grp", "ep", "tp"), None),
            P(("grp", "ep", "tp"), None),
            P(),
            P(("ep", "tp"), None, None),
            P(("ep", "tp"), None, None),
            P(("ep", "tp"), None, None),
        ),
        out_specs=P(("grp", "ep", "tp"), None),
        check_vma=False,
    )
```

```python
import functools

import jax
import jax.numpy as jnp
from jax import lax
from jax.experimental import pallas as pl
from jax.experimental.pallas import tpu as pltpu
from jax.sharding import PartitionSpec as P

MESH = pl.DeviceIdType.MESH
BF = jnp.bfloat16
F32 = jnp.float32
I32 = jnp.int32
Q = 4


def mm(a, b):
    return jnp.dot(a, b, preferred_element_type=F32)


def mm_nt(a, b):
    return lax.dot_general(a, b, (((1,), (1,)), ((), ())), preferred_element_type=F32)


class Dims:
    def __init__(self, ep, tp, tokens, width, fe, cap):
        self.NZ, self.NX = ep // 2, tp
        self.T, self.D, self.FE, self.CAP = tokens, width, fe, cap
        self.DQ = width // Q
        self.H = self.NZ // 2
        self.PL = 2 * tp
        self.RB = Q * cap
        self.NR = self.PL * self.RB
        self.SR = self.PL * 2 * cap
        plane = self.PL * cap
        self.caps = [tokens] + [
            min(tokens, (self.H - k) * plane + plane // 2) for k in range(1, self.H + 1)
        ]
        packed = [k for k in range(1, self.H + 1) if self.caps[k] < tokens]
        self.KP = packed[0] if packed else self.H + 1


def kernel(
    dm, hid_in, ids_in, wts_in, gain_in, wg, wu, wd, out_ref,
    hid, idv, wtv, gain, out,
    xs, metas, zb, zp, rin, rout, stage, rows, ysend, yrecv,
    ex, cm, sm, st, erow, upper, perm_g, perm_s, acc, xb, gacc, uacc, hb, yb,
    wgv, wuv, wdv,
    i_sem, o_sem, w_sem, m_send, m_recv, z_send, z_recv, p_send, p_recv, y_send, y_recv, r_send, r_recv,
):
    NZ, NX, T, D, FE, CAP = dm.NZ, dm.NX, dm.T, dm.D, dm.FE, dm.CAP
    DQ, H, PL, RB, NR, SR, KP, caps = dm.DQ, dm.H, dm.PL, dm.RB, dm.NR, dm.SR, dm.KP, dm.caps
    ep, x = lax.axis_index("ep"), lax.axis_index("tp")
    z, c = ep // 2, ep % 2

    def at_z(other):
        return {"ep": other * 2 + c, "tp": x}

    def onward(direction):
        return at_z((z + 1 - 2 * direction + NZ) % NZ)

    def backward(direction):
        return at_z((z - 1 + 2 * direction + NZ) % NZ)

    def in_plane(j):
        dc, dx = j // NX, j % NX
        return {"ep": z * 2 + (c + dc) % 2, "tp": (x + dx) % NX}

    def mirror(j):
        return (j // NX) * NX + (NX - j % NX) % NX

    barrier = pltpu.get_barrier_semaphore()
    for direction in range(2):
        pl.semaphore_signal(barrier, inc=1, device_id=onward(direction), device_id_type=MESH)
    for j in range(1, PL):
        pl.semaphore_signal(barrier, inc=1, device_id=in_plane(j), device_id_type=MESH)

    small_copies = [
        pltpu.make_async_copy(ids_in, idv, i_sem.at[0]),
        pltpu.make_async_copy(wts_in, wtv, i_sem.at[1]),
        pltpu.make_async_copy(gain_in, gain, i_sem.at[2]),
    ]
    part = T // 4
    hid_copies = [
        pltpu.make_async_copy(hid_in.at[pl.ds(i * part, part)], hid.at[pl.ds(i * part, part)], i_sem.at[3 + i])
        for i in range(4)
    ]
    for copy in [small_copies[2]] + hid_copies + small_copies[:2]:
        copy.start()
    weight_copies = []
    for q in range(Q):
        weight_copies.append(pltpu.make_async_copy(wg.at[0, pl.ds(q * DQ, DQ)], wgv.at[q], w_sem.at[0, q]))
        weight_copies.append(pltpu.make_async_copy(wu.at[0, pl.ds(q * DQ, DQ)], wuv.at[q], w_sem.at[1, q]))
        weight_copies.append(pltpu.make_async_copy(wd.at[0, :, pl.ds(q * DQ, DQ)], wdv.at[q], w_sem.at[2, q]))
    for copy in weight_copies:
        copy.start()

    r_id = lax.broadcasted_iota(I32, (NR, T), 0)
    j_id = r_id // RB
    dx_id, dc_id = j_id % NX, j_id // NX
    erow[...] = z * PL + ((c + dc_id) % 2) * NX + (x + dx_id) % NX
    slot_row = lax.broadcasted_iota(I32, (NR, T), 0) % CAP
    t_row = lax.broadcasted_iota(I32, (T, T), 0)
    t_col = lax.broadcasted_iota(I32, (T, T), 1)
    upper[...] = jnp.where(t_row < t_col, 1.0, 0.0).astype(BF)
    PR = Q * SR
    a_id = lax.broadcasted_iota(I32, (PR, PR), 0)
    n_id = lax.broadcasted_iota(I32, (PR, PR), 1)
    q_of, m_of = a_id // SR, a_id % SR
    perm_g[...] = jnp.where(n_id == (m_of // CAP) * RB + q_of * CAP + m_of % CAP, 1.0, 0.0).astype(BF)
    q_of, m_of = n_id // SR, n_id % SR
    perm_s[...] = jnp.where(a_id == (m_of // CAP) * RB + q_of * CAP + m_of % CAP, 1.0, 0.0).astype(BF)

    small_copies[2].wait()
    NB = min(16, part)

    def norm_rows(b, _):
        r = pl.ds(pl.multiple_of(b * NB, NB), NB)
        v = hid[r, :].astype(F32)
        scale = lax.rsqrt(jnp.mean(v * v, axis=-1, keepdims=True) + 1e-06)
        n = ((v * scale) * gain[...]).astype(BF)
        for q in range(Q):
            xs[q, r, :] = n[:, q * DQ:(q + 1) * DQ]
        return 0

    for i in range(4):
        hid_copies[i].wait()
        lax.fori_loop(i * (part // NB), (i + 1) * (part // NB), norm_rows, 0)

    small_copies[0].wait()
    small_copies[1].wait()
    for direction in range(2):
        metas[direction, 0, 0:2, :] = idv[...].astype(F32)
        metas[direction, 0, 2:4, :] = wtv[...]

    def z_copy(src, direction, k, q, rows_sent):
        return pltpu.make_async_remote_copy(
            src_ref=src, dst_ref=zb.at[direction, k - 1, q, pl.ds(0, rows_sent)],
            send_sem=z_send.at[direction, k - 1, q], recv_sem=z_recv.at[direction, k - 1, q],
            device_id=onward(direction), device_id_type=MESH,
        )

    def m_copy(direction, k):
        return pltpu.make_async_remote_copy(
            src_ref=metas.at[direction, k - 1], dst_ref=metas.at[direction, k],
            send_sem=m_send.at[direction, k], recv_sem=m_recv.at[direction, k],
            device_id=onward(direction), device_id_type=MESH,
        )

    def relay_meta(direction, k):
        m_copy(direction, k).wait_recv()
        if k < H:
            m_copy(direction, k + 1).start()

    relay_at = {(2, 3): 3, (3, 1): 4, (3, 3): 5, (4, 1): 6, (4, 3): 7, (5, 1): 8}
    assert H <= 8

    def plane_copy(src, dst, t, j, send, recv):
        if t < H:
            here, there = src.at[t - 1, j], dst.at[t - 1, mirror(j)]
        else:
            here, there = src.at[H - 1, j, t - H], dst.at[H - 1, mirror(j), t - H]
        return pltpu.make_async_remote_copy(
            src_ref=here, dst_ref=there, send_sem=send.at[t - 1, j], recv_sem=recv.at[t - 1, mirror(j)],
            device_id=in_plane(j), device_id_type=MESH,
        )

    def plane_start(src, dst, t, send, recv):
        for j in range(1, PL):
            plane_copy(src, dst, t, j, send, recv).start()

    def plane_wait(src, dst, t, send, recv):
        for j in range(1, PL):
            plane_copy(src, dst, t, mirror(j), send, recv).wait_recv()

    def plane_sent(src, dst, t, send, recv):
        for j in range(1, PL):
            plane_copy(src, dst, t, j, send, recv).wait_send()

    def build(direction, k):
        s = (z + NZ - k + 2 * k * direction) % NZ
        m = metas[direction, k]
        ids = [m[i:i + 1, :].astype(I32) for i in range(2)]
        wts = [m[2 + i:3 + i, :] for i in range(2)]
        e = erow[...]
        hit0, hit1 = e == ids[0], e == ids[1]
        hit = jnp.where(hit0, 1.0, 0.0) + jnp.where(hit1, 1.0, 0.0)
        count = mm(hit.astype(BF), upper[...])
        last = jnp.where(k == H, 1, 0)
        other_way = last * jnp.where(e % 2 == direction, 0, 1)
        sel = jnp.where(count == slot_row.astype(F32), hit, 0.0)
        sel = jnp.where(other_way == 1, 0.0, sel)
        pick = sel.astype(BF)
        weighted = ((jnp.where(hit0, wts[0], 0.0) + jnp.where(hit1, wts[1], 0.0)) * sel).astype(BF)

        reach = jnp.zeros((1, T), I32)
        for i in range(2):
            dist = ids[i] // PL - s
            dist = jnp.where(dist < 0, dist + NZ, dist)
            odd = ids[i] % 2
            up_way = jnp.where(dist < H, dist, jnp.where((dist == H) & (odd == 0), H, 0))
            down_way = jnp.where(dist > H, NZ - dist, jnp.where((dist == H) & (odd == 1), H, 0))
            reach = jnp.maximum(reach, jnp.where(direction == 0, up_way, down_way))

        def place(kk):
            mask = jnp.where(reach >= kk, 1.0, 0.0)
            pos = mm(jnp.broadcast_to(mask, (8, T)).astype(BF), upper[...])[0:1, :].astype(I32)
            pos = jnp.where(reach >= kk, pos, -1)
            col = lax.broadcasted_iota(I32, (1, T), 1)
            pos = jnp.where(kk >= KP, pos, col)
            return jnp.where(t_row == pos, 1.0, 0.0).astype(BF)

        here, after = place(k), place(k + 1)
        ex[direction, k] = mm_nt(pick, here).astype(BF)
        cm[direction, k] = mm_nt(here, weighted).astype(BF)
        sm[direction, k] = mm_nt(after, here).astype(BF)
        st[direction, k] = mm_nt(here, after).astype(BF)

    def build_steps(lo, hi):
        def one(i, _):
            build(i % 2, lo + i // 2)
            return 0

        lax.fori_loop(0, 2 * (hi - lo), one, 0)

    q_row = (lax.broadcasted_iota(I32, (NR, 1), 0) // CAP) % Q

    def only_q_rows(v, q):
        return jnp.where(q_row == q, v.astype(F32), 0.0).astype(BF)

    q_col = (lax.broadcasted_iota(I32, (1, NR), 1) // CAP) % Q

    def only_q_cols(v, q):
        return jnp.where(q_col == q, v.astype(F32), 0.0).astype(BF)

    def own_block():
        build(0, 0)
        acc[0] = jnp.zeros((NR, DQ), F32)

        def one(q, _):
            acc[0] = acc[0] + mm(only_q_rows(ex[0, 0], q), xs[q])
            return 0

        lax.fori_loop(0, Q, one, 0)
        own = acc[0].astype(BF).reshape(PL, RB, DQ)
        stage[H - 1, :, 1] = own
        rows[H - 1, 0, 1] = own[0]
        plane_start(stage, rows, H + 1, p_send, p_recv)

    def gather(k0):
        for i in range(2):
            k = k0 + i
            plane_wait(stage, rows, k, p_send, p_recv)
            if k == H:
                plane_wait(stage, rows, H + 1, p_send, p_recv)
            got = mm(perm_g[...], rows[k - 1].reshape(PR, DQ)).astype(BF).reshape(Q, SR, DQ)
            xb[:, pl.ds(i * SR, SR), :] = got
        gacc[...] = jnp.zeros_like(gacc)
        uacc[...] = jnp.zeros_like(uacc)

    def piece(i):
        @pl.when(i < Q)
        def _():
            gacc[...] += mm(xb[i], wgv[i])
            uacc[...] += mm(xb[i], wuv[i])

        @pl.when(i == Q)
        def _():
            g = gacc[...]
            hb[...] = ((g / (1.0 + jnp.exp(-g))) * uacc[...]).astype(BF)

        @pl.when(i >= Q)
        def _():
            yb[i - Q] = mm(hb[...], wdv[i - Q]).astype(BF)

    def scatter(k0):
        for i in range(2):
            k = k0 + i
            v = yb[:, pl.ds(i * SR, SR), :].reshape(PR, DQ)
            v = mm(perm_s[...], v).astype(BF).reshape(PL, 2, RB, DQ)
            ysend[k - 1] = v
            yrecv[k - 1, 0] = v[0]

    def experts(k0):
        gather(k0)

        def one(i, _):
            piece(i)
            return 0

        lax.fori_loop(0, 2 * Q, one, 0)
        scatter(k0)

    def dispatch(k, beside):
        ck = caps[k]
        acc[...] = jnp.zeros_like(acc)

        def chunk(i, _):
            q, direction = i // 2, i % 2
            for at_q in range(Q):
                if relay_at.get((k, at_q), H + 1) <= H:
                    @pl.when(q == at_q)
                    def _():
                        relay_meta(direction, relay_at[k, at_q])
            z_copy(zb.at[direction, k - 1, q, pl.ds(0, ck)], direction, k, q, ck).wait_recv()
            data = zb[direction, k - 1, q, pl.ds(0, ck), :]
            if k < H:
                cn = caps[k + 1]
                if k + 1 >= KP:
                    p = k + 1 - KP
                    zp[direction, p, q, pl.ds(0, cn), :] = mm(sm[direction, k][:cn, :ck], data).astype(BF)
                    source = zp.at[direction, p, q, pl.ds(0, cn)]
                else:
                    source = zb.at[direction, k - 1, q, pl.ds(0, cn)]
                z_copy(source, direction, k + 1, q, cn).start()
            e = only_q_rows(ex[direction, k], q)
            if ck < T:
                e = e[:, :ck]
            block = direction if k < H else 0
            acc[block] = acc[block] + mm(e, data)
            if beside:
                piece(i)
            return 0

        lax.fori_loop(0, 2 * Q, chunk, 0)
        for block in range(2 if k < H else 1):
            v = acc[block].astype(BF).reshape(PL, RB, DQ)
            stage[k - 1, :, block] = v
            rows[k - 1, 0, block] = v[0]
        plane_start(stage, rows, k, p_send, p_recv)

    firsts = list(range(1, H, 2))
    beside = {k0 + 3: k0 for k0 in firsts if k0 + 3 <= H - 2}
    after = [k0 for k0 in firsts if k0 + 3 > H - 2]
    sent = []

    pl.semaphore_wait(barrier, 2 + PL - 1)
    for direction in range(2):
        m_copy(direction, 1).start()
    for q in range(Q):
        for direction in range(2):
            z_copy(xs.at[q], direction, 1, q, caps[1]).start()
    own_block()
    for direction in range(2):
        relay_meta(direction, 1)
    build_steps(1, 2)
    dispatch(1, False)
    for direction in range(2):
        if H > 1:
            relay_meta(direction, 2)
    build_steps(2, min(3, H + 1))
    for copy in weight_copies:
        copy.wait()
    builds_after = {2: (3, 4), 3: (4, 6), 4: (6, 8), 5: (8, 9)}
    for k in range(2, H + 1):
        if k in beside:
            gather(beside[k])
        dispatch(k, k in beside)
        if k in beside:
            scatter(beside[k])
            if k < KP:
                sent.append(beside[k])
                for i in range(2):
                    plane_start(ysend, yrecv, beside[k] + i, y_send, y_recv)
        lo, hi = builds_after.get(k, (H + 1, H + 1))
        if lo <= H:
            build_steps(lo, min(hi, H + 1))
    for k0 in after:
        experts(k0)
    for k in range(H, after[0] - 1, -1):
        plane_start(ysend, yrecv, k, y_send, y_recv)
    for k0 in reversed([k0 for k0 in beside.values() if k0 not in sent]):
        for i in (1, 0):
            plane_start(ysend, yrecv, k0 + i, y_send, y_recv)
    plane_start(ysend, yrecv, H + 1, y_send, y_recv)

    def r_copy(direction, k, q):
        return pltpu.make_async_remote_copy(
            src_ref=rout.at[direction, k - 1, q, pl.ds(0, caps[k])],
            dst_ref=rin.at[direction, k - 1, q, pl.ds(0, caps[k])],
            send_sem=r_send.at[direction, k - 1, q], recv_sem=r_recv.at[direction, k - 1, q],
            device_id=backward(direction), device_id_type=MESH,
        )

    for k in range(H, 0, -1):
        ck = caps[k]
        plane_wait(ysend, yrecv, k, y_send, y_recv)

        def back(i, _, k=k, ck=ck):
            q, direction = i // 2, i % 2
            block = direction if k < H else 0
            y = yrecv[k - 1, :, block].reshape(NR, DQ)
            v = mm(only_q_cols(cm[direction, k, pl.ds(0, ck), :], q), y)
            if k < H:
                cn = caps[k + 1]
                r_copy(direction, k + 1, q).wait_recv()
                far = rin[direction, k, q, pl.ds(0, cn), :]
                if k + 1 >= KP:
                    v = v + mm(st[direction, k][:ck, :cn], far)
                else:
                    v = v + far.astype(F32)
            rout[direction, k - 1, q, pl.ds(0, ck), :] = v.astype(BF)
            r_copy(direction, k, q).start()
            z_copy(xs.at[q, pl.ds(0, ck)], direction, k, q, ck).wait_send()
            if k < H:
                r_copy(direction, k + 1, q).wait_send()
            return 0

        lax.fori_loop(0, 2 * Q, back, 0)
        plane_sent(stage, rows, k, p_send, p_recv)
        plane_sent(ysend, yrecv, k, y_send, y_recv)
        for direction in range(2):
            m_copy(direction, k).wait_send()

    plane_sent(stage, rows, H + 1, p_send, p_recv)
    plane_sent(ysend, yrecv, H + 1, y_send, y_recv)
    plane_wait(ysend, yrecv, H + 1, y_send, y_recv)

    def out_copy(q):
        return pltpu.make_async_copy(out.at[q], out_ref.at[:, pl.ds(q * DQ, DQ)], o_sem.at[q])

    y_own = yrecv[H - 1, :, 1].reshape(NR, DQ)
    for q in range(Q):
        v = mm(only_q_cols(cm[0, 0], q), y_own)
        for direction in range(2):
            r_copy(direction, 1, q).wait_recv()
            v = v + rin[direction, 0, q].astype(F32)
        out[q] = v.astype(BF)
        out_copy(q).start()
    for q in range(Q):
        for direction in range(2):
            r_copy(direction, 1, q).wait_send()
        out_copy(q).wait()


def body(hidden_in, expert_ids, route_weights, norm_gain, gate_proj, up_proj, down_proj):
    tokens, width = hidden_in.shape
    chosen = expert_ids.shape[1]
    ep, tp = lax.axis_size("ep"), lax.axis_size("tp")
    fe = gate_proj.shape[2]
    cap = max(2, 2 * chosen * tokens // (ep * tp))
    dm = Dims(ep, tp, tokens, width, fe, cap)
    H, T, DQ, PL, RB, NR, SR = dm.H, dm.T, dm.DQ, dm.PL, dm.RB, dm.NR, dm.SR
    vm = pltpu.VMEM
    packed = max(1, H - dm.KP + 1)
    dma = pltpu.SemaphoreType.DMA
    return pl.pallas_call(
        functools.partial(kernel, dm),
        out_shape=jax.ShapeDtypeStruct((tokens, width), BF),
        in_specs=[pl.BlockSpec(memory_space=pl.ANY)] * 7,
        out_specs=pl.BlockSpec(memory_space=pl.ANY),
        scratch_shapes=[
            vm((tokens, width), BF),
            vm((2, tokens), I32),
            vm((2, tokens), F32),
            vm((1, width), F32),
            vm((Q, T, DQ), BF),
            vm((Q, T, DQ), BF),
            vm((2, H + 1, 4, T), F32),
            vm((2, H, Q, T, DQ), BF),
            vm((2, packed, Q, dm.caps[min(dm.KP, H)], DQ), BF),
            vm((2, H, Q, T, DQ), BF),
            vm((2, H, Q, T, DQ), BF),
            vm((H, PL, 2, RB, DQ), BF),
            vm((H, PL, 2, RB, DQ), BF),
            vm((H, PL, 2, RB, DQ), BF),
            vm((H, PL, 2, RB, DQ), BF),
            vm((2, H + 1, NR, T), BF),
            vm((2, H + 1, T, NR), BF),
            vm((2, H + 1, T, T), BF),
            vm((2, H + 1, T, T), BF),
            vm((NR, T), I32),
            vm((T, T), BF),
            vm((Q * SR, Q * SR), BF),
            vm((Q * SR, Q * SR), BF),
            vm((2, NR, DQ), F32),
            vm((Q, 2 * SR, DQ), BF),
            vm((2 * SR, fe), F32),
            vm((2 * SR, fe), F32),
            vm((2 * SR, fe), BF),
            vm((Q, 2 * SR, DQ), BF),
            vm((Q, DQ, fe), BF),
            vm((Q, DQ, fe), BF),
            vm((Q, fe, DQ), BF),
            dma((7,)),
            dma((Q,)),
            dma((3, Q)),
            dma((2, H + 1)),
            dma((2, H + 1)),
            dma((2, H, Q)),
            dma((2, H, Q)),
            dma((H + 1, PL)),
            dma((H + 1, PL)),
            dma((H + 1, PL)),
            dma((H + 1, PL)),
            dma((2, H, Q)),
            dma((2, H, Q)),
        ],
        compiler_params=pltpu.CompilerParams(
            collective_id=0, has_side_effects=True, vmem_limit_bytes=66 * 1000 * 1000
        ),
        name="routed_experts",
    )(hidden_in, expert_ids.T, route_weights.T, norm_gain.reshape(1, width), gate_proj, up_proj, down_proj)


def solution(mesh):
    return jax.shard_map(
        body,
        mesh=mesh,
        in_specs=(
            P(("grp", "ep", "tp"), None),
            P(("grp", "ep", "tp"), None),
            P(("grp", "ep", "tp"), None),
            P(),
            P(("ep", "tp"), None, None),
            P(("ep", "tp"), None, None),
            P(("ep", "tp"), None, None),
        ),
        out_specs=P(("grp", "ep", "tp"), None),
        check_vma=False,
    )
```

```python
import functools

import jax
import jax.numpy as jnp
from jax import lax
from jax.experimental import pallas as pl
from jax.experimental.pallas import tpu as pltpu
from jax.sharding import PartitionSpec as P

MESH = pl.DeviceIdType.MESH
BF = jnp.bfloat16
F32 = jnp.float32
I32 = jnp.int32
Q = 4


def mm(a, b):
    return jnp.dot(a, b, preferred_element_type=F32)


def mm_nt(a, b):
    return lax.dot_general(a, b, (((1,), (1,)), ((), ())), preferred_element_type=F32)


class Dims:
    def __init__(self, ep, tp, tokens, width, fe, cap):
        self.NZ, self.NX = ep // 2, tp
        self.T, self.D, self.FE, self.CAP = tokens, width, fe, cap
        self.DQ = width // Q
        self.H = self.NZ // 2
        self.PL = 2 * tp
        self.RB = Q * cap
        self.NR = self.PL * self.RB
        self.SR = self.PL * 2 * cap
        plane = self.PL * cap
        self.caps = [tokens] + [
            min(tokens, (self.H - k) * plane + plane // 2) for k in range(1, self.H + 1)
        ]
        packed = [k for k in range(1, self.H + 1) if self.caps[k] < tokens]
        self.KP = packed[0] if packed else self.H + 1


def kernel(
    dm, hid_in, ids_in, wts_in, gain_in, wg, wu, wd, out_ref,
    hid, idv, wtv, gain, out,
    xs, metas, zb, zp, rin, rout, stage, rows, ysend, yrecv,
    ex, cm, sm, st, erow, upper, perm_g, perm_s, acc, xb, gacc, uacc, hb, yb,
    wgv, wuv, wdv,
    i_sem, o_sem, w_sem, m_send, m_recv, z_send, z_recv, p_send, p_recv, y_send, y_recv, r_send, r_recv,
):
    NZ, NX, T, D, FE, CAP = dm.NZ, dm.NX, dm.T, dm.D, dm.FE, dm.CAP
    DQ, H, PL, RB, NR, SR, KP, caps = dm.DQ, dm.H, dm.PL, dm.RB, dm.NR, dm.SR, dm.KP, dm.caps
    ep, x = lax.axis_index("ep"), lax.axis_index("tp")
    z, c = ep // 2, ep % 2

    def at_z(other):
        return {"ep": other * 2 + c, "tp": x}

    def onward(direction):
        return at_z((z + 1 - 2 * direction + NZ) % NZ)

    def backward(direction):
        return at_z((z - 1 + 2 * direction + NZ) % NZ)

    def in_plane(j):
        dc, dx = j // NX, j % NX
        return {"ep": z * 2 + (c + dc) % 2, "tp": (x + dx) % NX}

    def mirror(j):
        return (j // NX) * NX + (NX - j % NX) % NX

    barrier = pltpu.get_barrier_semaphore()
    for direction in range(2):
        pl.semaphore_signal(barrier, inc=1, device_id=onward(direction), device_id_type=MESH)
    for j in range(1, PL):
        pl.semaphore_signal(barrier, inc=1, device_id=in_plane(j), device_id_type=MESH)

    small_copies = [
        pltpu.make_async_copy(ids_in, idv, i_sem.at[0]),
        pltpu.make_async_copy(wts_in, wtv, i_sem.at[1]),
        pltpu.make_async_copy(gain_in, gain, i_sem.at[2]),
    ]
    part = T // 4
    hid_copies = [
        pltpu.make_async_copy(hid_in.at[pl.ds(i * part, part)], hid.at[pl.ds(i * part, part)], i_sem.at[3 + i])
        for i in range(4)
    ]
    for copy in [small_copies[2]] + hid_copies + small_copies[:2]:
        copy.start()
    weight_copies = []
    for q in range(Q):
        weight_copies.append(pltpu.make_async_copy(wg.at[0, pl.ds(q * DQ, DQ)], wgv.at[q], w_sem.at[0, q]))
        weight_copies.append(pltpu.make_async_copy(wu.at[0, pl.ds(q * DQ, DQ)], wuv.at[q], w_sem.at[1, q]))
        weight_copies.append(pltpu.make_async_copy(wd.at[0, :, pl.ds(q * DQ, DQ)], wdv.at[q], w_sem.at[2, q]))
    r_id = lax.broadcasted_iota(I32, (NR, T), 0)
    j_id = r_id // RB
    dx_id, dc_id = j_id % NX, j_id // NX
    erow[...] = z * PL + ((c + dc_id) % 2) * NX + (x + dx_id) % NX
    slot_row = lax.broadcasted_iota(I32, (NR, T), 0) % CAP
    t_row = lax.broadcasted_iota(I32, (T, T), 0)
    t_col = lax.broadcasted_iota(I32, (T, T), 1)
    upper[...] = jnp.where(t_row < t_col, 1.0, 0.0).astype(BF)
    PR = Q * SR
    a_id = lax.broadcasted_iota(I32, (PR, PR), 0)
    n_id = lax.broadcasted_iota(I32, (PR, PR), 1)
    q_of, m_of = a_id // SR, a_id % SR
    perm_g[...] = jnp.where(n_id == (m_of // CAP) * RB + q_of * CAP + m_of % CAP, 1.0, 0.0).astype(BF)
    q_of, m_of = n_id // SR, n_id % SR
    perm_s[...] = jnp.where(a_id == (m_of // CAP) * RB + q_of * CAP + m_of % CAP, 1.0, 0.0).astype(BF)

    small_copies[2].wait()
    NB = min(16, part)

    def norm_rows(b, _):
        r = pl.ds(pl.multiple_of(b * NB, NB), NB)
        v = hid[r, :].astype(F32)
        scale = lax.rsqrt(jnp.mean(v * v, axis=-1, keepdims=True) + 1e-06)
        n = ((v * scale) * gain[...]).astype(BF)
        for q in range(Q):
            xs[q, r, :] = n[:, q * DQ:(q + 1) * DQ]
        return 0

    for i in range(4):
        hid_copies[i].wait()
        lax.fori_loop(i * (part // NB), (i + 1) * (part // NB), norm_rows, 0)

    small_copies[0].wait()
    small_copies[1].wait()
    for direction in range(2):
        metas[direction, 0, 0:2, :] = idv[...].astype(F32)
        metas[direction, 0, 2:4, :] = wtv[...]

    def z_copy(src, direction, k, q, rows_sent):
        return pltpu.make_async_remote_copy(
            src_ref=src, dst_ref=zb.at[direction, k - 1, q, pl.ds(0, rows_sent)],
            send_sem=z_send.at[direction, k - 1, q], recv_sem=z_recv.at[direction, k - 1, q],
            device_id=onward(direction), device_id_type=MESH,
        )

    def m_copy(direction, k):
        return pltpu.make_async_remote_copy(
            src_ref=metas.at[direction, k - 1], dst_ref=metas.at[direction, k],
            send_sem=m_send.at[direction, k], recv_sem=m_recv.at[direction, k],
            device_id=onward(direction), device_id_type=MESH,
        )

    def relay_meta(direction, k):
        m_copy(direction, k).wait_recv()
        if k < H:
            m_copy(direction, k + 1).start()

    relay_at = {(1, 3): 2, (2, 2): 3, (3, 1): 4, (4, 0): 5, (4, 3): 6, (5, 2): 7, (6, 1): 8}
    assert H <= 8

    def plane_copy(src, dst, t, j, send, recv):
        if t < H:
            here, there = src.at[t - 1, j], dst.at[t - 1, mirror(j)]
        else:
            here, there = src.at[H - 1, j, t - H], dst.at[H - 1, mirror(j), t - H]
        return pltpu.make_async_remote_copy(
            src_ref=here, dst_ref=there, send_sem=send.at[t - 1, j], recv_sem=recv.at[t - 1, mirror(j)],
            device_id=in_plane(j), device_id_type=MESH,
        )

    def plane_start(src, dst, t, send, recv):
        for j in range(1, PL):
            plane_copy(src, dst, t, j, send, recv).start()

    def plane_wait(src, dst, t, send, recv):
        for j in range(1, PL):
            plane_copy(src, dst, t, mirror(j), send, recv).wait_recv()

    def plane_sent(src, dst, t, send, recv):
        for j in range(1, PL):
            plane_copy(src, dst, t, j, send, recv).wait_send()

    def build(direction, k):
        s = (z + NZ - k + 2 * k * direction) % NZ
        m = metas[direction, k]
        ids = [m[i:i + 1, :].astype(I32) for i in range(2)]
        wts = [m[2 + i:3 + i, :] for i in range(2)]
        e = erow[...]
        hit0, hit1 = e == ids[0], e == ids[1]
        hit = jnp.where(hit0, 1.0, 0.0) + jnp.where(hit1, 1.0, 0.0)
        count = mm(hit.astype(BF), upper[...])
        last = jnp.where(k == H, 1, 0)
        other_way = last * jnp.where(e % 2 == direction, 0, 1)
        sel = jnp.where(count == slot_row.astype(F32), hit, 0.0)
        sel = jnp.where(other_way == 1, 0.0, sel)
        pick = sel.astype(BF)
        weighted = ((jnp.where(hit0, wts[0], 0.0) + jnp.where(hit1, wts[1], 0.0)) * sel).astype(BF)

        reach = jnp.zeros((1, T), I32)
        for i in range(2):
            dist = ids[i] // PL - s
            dist = jnp.where(dist < 0, dist + NZ, dist)
            odd = ids[i] % 2
            up_way = jnp.where(dist < H, dist, jnp.where((dist == H) & (odd == 0), H, 0))
            down_way = jnp.where(dist > H, NZ - dist, jnp.where((dist == H) & (odd == 1), H, 0))
            reach = jnp.maximum(reach, jnp.where(direction == 0, up_way, down_way))

        def place(kk):
            mask = jnp.where(reach >= kk, 1.0, 0.0)
            pos = mm(jnp.broadcast_to(mask, (8, T)).astype(BF), upper[...])[0:1, :].astype(I32)
            pos = jnp.where(reach >= kk, pos, -1)
            col = lax.broadcasted_iota(I32, (1, T), 1)
            pos = jnp.where(kk >= KP, pos, col)
            return jnp.where(t_row == pos, 1.0, 0.0).astype(BF)

        here, after = place(k), place(k + 1)
        ex[direction, k] = mm_nt(pick, here).astype(BF)
        cm[direction, k] = mm_nt(here, weighted).astype(BF)
        sm[direction, k] = mm_nt(after, here).astype(BF)
        st[direction, k] = mm_nt(here, after).astype(BF)

    def build_steps(lo, hi):
        def one(i, _):
            build(i % 2, lo + i // 2)
            return 0

        lax.fori_loop(0, 2 * (hi - lo), one, 0)

    q_row = (lax.broadcasted_iota(I32, (NR, 1), 0) // CAP) % Q

    def only_q_rows(v, q):
        return jnp.where(q_row == q, v.astype(F32), 0.0).astype(BF)

    q_col = (lax.broadcasted_iota(I32, (1, NR), 1) // CAP) % Q

    def only_q_cols(v, q):
        return jnp.where(q_col == q, v.astype(F32), 0.0).astype(BF)

    def own_block():
        build(0, 0)
        acc[0] = jnp.zeros((NR, DQ), F32)

        def one(q, _):
            acc[0] = acc[0] + mm(only_q_rows(ex[0, 0], q), xs[q])
            return 0

        lax.fori_loop(0, Q, one, 0)
        own = acc[0].astype(BF).reshape(PL, RB, DQ)
        stage[H - 1, :, 1] = own
        rows[H - 1, 0, 1] = own[0]
        plane_start(stage, rows, H + 1, p_send, p_recv)

    def gather(k0):
        for i in range(2):
            k = k0 + i
            plane_wait(stage, rows, k, p_send, p_recv)
            if k == H:
                plane_wait(stage, rows, H + 1, p_send, p_recv)
            got = mm(perm_g[...], rows[k - 1].reshape(PR, DQ)).astype(BF).reshape(Q, SR, DQ)
            xb[:, pl.ds(i * SR, SR), :] = got
        gacc[...] = jnp.zeros_like(gacc)
        uacc[...] = jnp.zeros_like(uacc)

    def piece(i):
        @pl.when(i < Q)
        def _():
            gacc[...] += mm(xb[i], wgv[i])
            uacc[...] += mm(xb[i], wuv[i])

        @pl.when(i == Q)
        def _():
            g = gacc[...]
            hb[...] = ((g / (1.0 + jnp.exp(-g))) * uacc[...]).astype(BF)

        @pl.when(i >= Q)
        def _():
            yb[i - Q] = mm(hb[...], wdv[i - Q]).astype(BF)

    def scatter(k0):
        for i in range(2):
            k = k0 + i
            v = yb[:, pl.ds(i * SR, SR), :].reshape(PR, DQ)
            v = mm(perm_s[...], v).astype(BF).reshape(PL, 2, RB, DQ)
            ysend[k - 1] = v
            yrecv[k - 1, 0] = v[0]

    def experts(k0):
        gather(k0)

        def one(i, _):
            piece(i)
            return 0

        lax.fori_loop(0, 2 * Q, one, 0)
        scatter(k0)

    def dispatch(k, beside):
        ck = caps[k]
        acc[...] = jnp.zeros_like(acc)

        def chunk(i, _):
            q, direction = i // 2, i % 2
            for at_q in range(Q):
                if relay_at.get((k, at_q), H + 1) <= H:
                    @pl.when(q == at_q)
                    def _():
                        relay_meta(direction, relay_at[k, at_q])
            z_copy(zb.at[direction, k - 1, q, pl.ds(0, ck)], direction, k, q, ck).wait_recv()
            data = zb[direction, k - 1, q, pl.ds(0, ck), :]
            if k < H:
                cn = caps[k + 1]
                if k + 1 >= KP:
                    p = k + 1 - KP
                    zp[direction, p, q, pl.ds(0, cn), :] = mm(sm[direction, k][:cn, :ck], data).astype(BF)
                    source = zp.at[direction, p, q, pl.ds(0, cn)]
                else:
                    source = zb.at[direction, k - 1, q, pl.ds(0, cn)]
                z_copy(source, direction, k + 1, q, cn).start()
            e = only_q_rows(ex[direction, k], q)
            if ck < T:
                e = e[:, :ck]
            block = direction if k < H else 0
            acc[block] = acc[block] + mm(e, data)
            if beside:
                piece(i)
            return 0

        lax.fori_loop(0, 2 * Q, chunk, 0)
        for block in range(2 if k < H else 1):
            v = acc[block].astype(BF).reshape(PL, RB, DQ)
            stage[k - 1, :, block] = v
            rows[k - 1, 0, block] = v[0]
        plane_start(stage, rows, k, p_send, p_recv)

    firsts = list(range(1, H, 2))
    beside = {k0 + 3: k0 for k0 in firsts if k0 + 3 <= H - 2}
    after = [k0 for k0 in firsts if k0 + 3 > H - 2]
    sent = []

    pl.semaphore_wait(barrier, 2 + PL - 1)
    for direction in range(2):
        m_copy(direction, 1).start()
    for q in range(Q):
        for direction in range(2):
            z_copy(xs.at[q], direction, 1, q, caps[1]).start()
    for copy in weight_copies:
        copy.start()
    own_block()
    for direction in range(2):
        relay_meta(direction, 1)
    build_steps(1, 2)
    dispatch(1, False)
    build_steps(2, min(3, H + 1))
    for copy in weight_copies:
        copy.wait()
    builds_after = {2: (3, 4), 3: (4, 5), 4: (5, 7), 5: (7, 8), 6: (8, 9)}
    for k in range(2, H + 1):
        if k in beside:
            gather(beside[k])
        dispatch(k, k in beside)
        if k in beside:
            scatter(beside[k])
            if k < KP:
                sent.append(beside[k])
                for i in range(2):
                    plane_start(ysend, yrecv, beside[k] + i, y_send, y_recv)
        lo, hi = builds_after.get(k, (H + 1, H + 1))
        if lo <= H:
            build_steps(lo, min(hi, H + 1))
    for k0 in after:
        experts(k0)
    for k in range(H, after[0] - 1, -1):
        plane_start(ysend, yrecv, k, y_send, y_recv)
    for k0 in reversed([k0 for k0 in beside.values() if k0 not in sent]):
        for i in (1, 0):
            plane_start(ysend, yrecv, k0 + i, y_send, y_recv)
    plane_start(ysend, yrecv, H + 1, y_send, y_recv)

    def r_copy(direction, k, q):
        return pltpu.make_async_remote_copy(
            src_ref=rout.at[direction, k - 1, q, pl.ds(0, caps[k])],
            dst_ref=rin.at[direction, k - 1, q, pl.ds(0, caps[k])],
            send_sem=r_send.at[direction, k - 1, q], recv_sem=r_recv.at[direction, k - 1, q],
            device_id=backward(direction), device_id_type=MESH,
        )

    for k in range(H, 0, -1):
        ck = caps[k]
        plane_wait(ysend, yrecv, k, y_send, y_recv)

        def back(i, _, k=k, ck=ck):
            q, direction = i // 2, i % 2
            block = direction if k < H else 0
            y = yrecv[k - 1, :, block].reshape(NR, DQ)
            v = mm(only_q_cols(cm[direction, k, pl.ds(0, ck), :], q), y)
            if k < H:
                cn = caps[k + 1]
                r_copy(direction, k + 1, q).wait_recv()
                far = rin[direction, k, q, pl.ds(0, cn), :]
                if k + 1 >= KP:
                    v = v + mm(st[direction, k][:ck, :cn], far)
                else:
                    v = v + far.astype(F32)
            rout[direction, k - 1, q, pl.ds(0, ck), :] = v.astype(BF)
            r_copy(direction, k, q).start()
            z_copy(xs.at[q, pl.ds(0, ck)], direction, k, q, ck).wait_send()
            if k < H:
                r_copy(direction, k + 1, q).wait_send()
            return 0

        lax.fori_loop(0, 2 * Q, back, 0)
        plane_sent(stage, rows, k, p_send, p_recv)
        plane_sent(ysend, yrecv, k, y_send, y_recv)
        for direction in range(2):
            m_copy(direction, k).wait_send()

    plane_sent(stage, rows, H + 1, p_send, p_recv)
    plane_sent(ysend, yrecv, H + 1, y_send, y_recv)
    plane_wait(ysend, yrecv, H + 1, y_send, y_recv)

    def out_copy(q):
        return pltpu.make_async_copy(out.at[q], out_ref.at[:, pl.ds(q * DQ, DQ)], o_sem.at[q])

    y_own = yrecv[H - 1, :, 1].reshape(NR, DQ)
    for q in range(Q):
        v = mm(only_q_cols(cm[0, 0], q), y_own)
        for direction in range(2):
            r_copy(direction, 1, q).wait_recv()
            v = v + rin[direction, 0, q].astype(F32)
        out[q] = v.astype(BF)
        out_copy(q).start()
    for q in range(Q):
        for direction in range(2):
            r_copy(direction, 1, q).wait_send()
        out_copy(q).wait()


def body(hidden_in, expert_ids, route_weights, norm_gain, gate_proj, up_proj, down_proj):
    tokens, width = hidden_in.shape
    chosen = expert_ids.shape[1]
    ep, tp = lax.axis_size("ep"), lax.axis_size("tp")
    fe = gate_proj.shape[2]
    cap = max(2, 2 * chosen * tokens // (ep * tp))
    dm = Dims(ep, tp, tokens, width, fe, cap)
    H, T, DQ, PL, RB, NR, SR = dm.H, dm.T, dm.DQ, dm.PL, dm.RB, dm.NR, dm.SR
    vm = pltpu.VMEM
    packed = max(1, H - dm.KP + 1)
    dma = pltpu.SemaphoreType.DMA
    return pl.pallas_call(
        functools.partial(kernel, dm),
        out_shape=jax.ShapeDtypeStruct((tokens, width), BF),
        in_specs=[pl.BlockSpec(memory_space=pl.ANY)] * 7,
        out_specs=pl.BlockSpec(memory_space=pl.ANY),
        scratch_shapes=[
            vm((tokens, width), BF),
            vm((2, tokens), I32),
            vm((2, tokens), F32),
            vm((1, width), F32),
            vm((Q, T, DQ), BF),
            vm((Q, T, DQ), BF),
            vm((2, H + 1, 4, T), F32),
            vm((2, H, Q, T, DQ), BF),
            vm((2, packed, Q, dm.caps[min(dm.KP, H)], DQ), BF),
            vm((2, H, Q, T, DQ), BF),
            vm((2, H, Q, T, DQ), BF),
            vm((H, PL, 2, RB, DQ), BF),
            vm((H, PL, 2, RB, DQ), BF),
            vm((H, PL, 2, RB, DQ), BF),
            vm((H, PL, 2, RB, DQ), BF),
            vm((2, H + 1, NR, T), BF),
            vm((2, H + 1, T, NR), BF),
            vm((2, H + 1, T, T), BF),
            vm((2, H + 1, T, T), BF),
            vm((NR, T), I32),
            vm((T, T), BF),
            vm((Q * SR, Q * SR), BF),
            vm((Q * SR, Q * SR), BF),
            vm((2, NR, DQ), F32),
            vm((Q, 2 * SR, DQ), BF),
            vm((2 * SR, fe), F32),
            vm((2 * SR, fe), F32),
            vm((2 * SR, fe), BF),
            vm((Q, 2 * SR, DQ), BF),
            vm((Q, DQ, fe), BF),
            vm((Q, DQ, fe), BF),
            vm((Q, fe, DQ), BF),
            dma((7,)),
            dma((Q,)),
            dma((3, Q)),
            dma((2, H + 1)),
            dma((2, H + 1)),
            dma((2, H, Q)),
            dma((2, H, Q)),
            dma((H + 1, PL)),
            dma((H + 1, PL)),
            dma((H + 1, PL)),
            dma((H + 1, PL)),
            dma((2, H, Q)),
            dma((2, H, Q)),
        ],
        compiler_params=pltpu.CompilerParams(
            collective_id=0, has_side_effects=True, vmem_limit_bytes=66 * 1000 * 1000
        ),
        name="routed_experts",
    )(hidden_in, expert_ids.T, route_weights.T, norm_gain.reshape(1, width), gate_proj, up_proj, down_proj)


def solution(mesh):
    return jax.shard_map(
        body,
        mesh=mesh,
        in_specs=(
            P(("grp", "ep", "tp"), None),
            P(("grp", "ep", "tp"), None),
            P(("grp", "ep", "tp"), None),
            P(),
            P(("ep", "tp"), None, None),
            P(("ep", "tp"), None, None),
            P(("ep", "tp"), None, None),
        ),
        out_specs=P(("grp", "ep", "tp"), None),
        check_vma=False,
    )
```

```python
import functools

import jax
import jax.numpy as jnp
from jax import lax
from jax.experimental import pallas as pl
from jax.experimental.pallas import tpu as pltpu
from jax.sharding import PartitionSpec as P

MESH = pl.DeviceIdType.MESH
BF = jnp.bfloat16
F32 = jnp.float32
I32 = jnp.int32
Q = 4


def mm(a, b):
    return jnp.dot(a, b, preferred_element_type=F32)


def mm_nt(a, b):
    return lax.dot_general(a, b, (((1,), (1,)), ((), ())), preferred_element_type=F32)


class Dims:
    def __init__(self, ep, tp, tokens, width, fe, cap):
        self.NZ, self.NX = ep // 2, tp
        self.T, self.D, self.FE, self.CAP = tokens, width, fe, cap
        self.DQ = width // Q
        self.H = self.NZ // 2
        self.PL = 2 * tp
        self.RB = Q * cap
        self.NR = self.PL * self.RB
        self.SR = self.PL * 2 * cap
        plane = self.PL * cap
        self.caps = [tokens] + [
            min(tokens, (self.H - k) * plane + plane // 2) for k in range(1, self.H + 1)
        ]
        packed = [k for k in range(1, self.H + 1) if self.caps[k] < tokens]
        self.KP = packed[0] if packed else self.H + 1


def kernel(
    dm, hid_in, ids_in, wts_in, gain_in, wg, wu, wd, out_ref,
    hid, idv, wtv, gain, out,
    xs, metas, zb, zp, rin, rout, stage, rows, ysend, yrecv,
    ex, cm, sm, st, erow, upper, perm_g, perm_s, acc, xb, gacc, uacc, hb, yb,
    wgv, wuv, wdv,
    i_sem, o_sem, w_sem, m_send, m_recv, z_send, z_recv, p_send, p_recv, y_send, y_recv, r_send, r_recv,
):
    NZ, NX, T, D, FE, CAP = dm.NZ, dm.NX, dm.T, dm.D, dm.FE, dm.CAP
    DQ, H, PL, RB, NR, SR, KP, caps = dm.DQ, dm.H, dm.PL, dm.RB, dm.NR, dm.SR, dm.KP, dm.caps
    ep, x = lax.axis_index("ep"), lax.axis_index("tp")
    z, c = ep // 2, ep % 2

    def at_z(other):
        return {"ep": other * 2 + c, "tp": x}

    def onward(direction):
        return at_z((z + 1 - 2 * direction + NZ) % NZ)

    def backward(direction):
        return at_z((z - 1 + 2 * direction + NZ) % NZ)

    def in_plane(j):
        dc, dx = j // NX, j % NX
        return {"ep": z * 2 + (c + dc) % 2, "tp": (x + dx) % NX}

    def mirror(j):
        return (j // NX) * NX + (NX - j % NX) % NX

    barrier = pltpu.get_barrier_semaphore()
    for direction in range(2):
        pl.semaphore_signal(barrier, inc=1, device_id=onward(direction), device_id_type=MESH)
    for j in range(1, PL):
        pl.semaphore_signal(barrier, inc=1, device_id=in_plane(j), device_id_type=MESH)

    small_copies = [
        pltpu.make_async_copy(ids_in, idv, i_sem.at[0]),
        pltpu.make_async_copy(wts_in, wtv, i_sem.at[1]),
        pltpu.make_async_copy(gain_in, gain, i_sem.at[2]),
    ]
    part = T // 4
    hid_copies = [
        pltpu.make_async_copy(hid_in.at[pl.ds(i * part, part)], hid.at[pl.ds(i * part, part)], i_sem.at[3 + i])
        for i in range(4)
    ]
    for copy in [small_copies[2]] + hid_copies + small_copies[:2]:
        copy.start()
    weight_copies = []
    for q in range(Q):
        weight_copies.append(pltpu.make_async_copy(wg.at[0, pl.ds(q * DQ, DQ)], wgv.at[q], w_sem.at[0, q]))
        weight_copies.append(pltpu.make_async_copy(wu.at[0, pl.ds(q * DQ, DQ)], wuv.at[q], w_sem.at[1, q]))
        weight_copies.append(pltpu.make_async_copy(wd.at[0, :, pl.ds(q * DQ, DQ)], wdv.at[q], w_sem.at[2, q]))
    r_id = lax.broadcasted_iota(I32, (NR, T), 0)
    j_id = r_id // RB
    dx_id, dc_id = j_id % NX, j_id // NX
    erow[...] = z * PL + ((c + dc_id) % 2) * NX + (x + dx_id) % NX
    slot_row = lax.broadcasted_iota(I32, (NR, T), 0) % CAP
    t_row = lax.broadcasted_iota(I32, (T, T), 0)
    t_col = lax.broadcasted_iota(I32, (T, T), 1)
    upper[...] = jnp.where(t_row < t_col, 1.0, 0.0).astype(BF)
    PR = Q * SR
    a_id = lax.broadcasted_iota(I32, (PR, PR), 0)
    n_id = lax.broadcasted_iota(I32, (PR, PR), 1)
    q_of, m_of = a_id // SR, a_id % SR
    perm_g[...] = jnp.where(n_id == (m_of // CAP) * RB + q_of * CAP + m_of % CAP, 1.0, 0.0).astype(BF)
    q_of, m_of = n_id // SR, n_id % SR
    perm_s[...] = jnp.where(a_id == (m_of // CAP) * RB + q_of * CAP + m_of % CAP, 1.0, 0.0).astype(BF)

    small_copies[2].wait()
    NB = min(16, part)

    def norm_rows(b, _):
        r = pl.ds(pl.multiple_of(b * NB, NB), NB)
        v = hid[r, :].astype(F32)
        scale = lax.rsqrt(jnp.mean(v * v, axis=-1, keepdims=True) + 1e-06)
        n = ((v * scale) * gain[...]).astype(BF)
        for q in range(Q):
            xs[q, r, :] = n[:, q * DQ:(q + 1) * DQ]
        return 0

    for i in range(4):
        hid_copies[i].wait()
        lax.fori_loop(i * (part // NB), (i + 1) * (part // NB), norm_rows, 0)

    small_copies[0].wait()
    small_copies[1].wait()
    for direction in range(2):
        metas[direction, 0, 0:2, :] = idv[...].astype(F32)
        metas[direction, 0, 2:4, :] = wtv[...]

    def z_copy(src, direction, k, q, rows_sent):
        return pltpu.make_async_remote_copy(
            src_ref=src, dst_ref=zb.at[direction, k - 1, q, pl.ds(0, rows_sent)],
            send_sem=z_send.at[k - 1], recv_sem=z_recv.at[direction, k - 1, q],
            device_id=onward(direction), device_id_type=MESH,
        )

    def m_copy(direction, k):
        return pltpu.make_async_remote_copy(
            src_ref=metas.at[direction, k - 1], dst_ref=metas.at[direction, k],
            send_sem=m_send.at[0], recv_sem=m_recv.at[direction, k],
            device_id=onward(direction), device_id_type=MESH,
        )

    def relay_meta(direction, k):
        m_copy(direction, k).wait_recv()
        if k < H:
            m_copy(direction, k + 1).start()

    relay_at = {(1, 3): 2, (2, 2): 3, (3, 1): 4, (4, 0): 5, (4, 3): 6, (5, 2): 7, (6, 1): 8}
    assert H <= 8

    def blocks(ref, t, j):
        return ref.at[t - 1, j] if t < H else ref.at[H - 1, j, t - H]

    def plane_copy(src, dst, t, j, to, send, recv):
        return pltpu.make_async_remote_copy(
            src_ref=blocks(src, t, j), dst_ref=blocks(dst, t, to), send_sem=send.at[t - 1], recv_sem=recv.at[t - 1],
            device_id=in_plane(1 if j is others else j), device_id_type=MESH,
        )

    others = pl.ds(1, PL - 1)

    def plane_start(src, dst, t, send, recv):
        for j in range(1, PL):
            plane_copy(src, dst, t, j, mirror(j), send, recv).start()

    def plane_wait(src, dst, t, send, recv):
        plane_copy(src, dst, t, others, others, send, recv).wait_recv()

    def plane_sent(src, dst, t, send, recv):
        plane_copy(src, dst, t, others, others, send, recv).wait_send()

    def all_sent(src, send, recv):
        pltpu.make_async_remote_copy(
            src_ref=src, dst_ref=src, send_sem=send, recv_sem=recv, device_id=onward(0), device_id_type=MESH
        ).wait_send()

    def build(direction, k):
        s = (z + NZ - k + 2 * k * direction) % NZ
        m = metas[direction, k]
        ids = [m[i:i + 1, :].astype(I32) for i in range(2)]
        wts = [m[2 + i:3 + i, :] for i in range(2)]
        e = erow[...]
        hit0, hit1 = e == ids[0], e == ids[1]
        hit = jnp.where(hit0, 1.0, 0.0) + jnp.where(hit1, 1.0, 0.0)
        count = mm(hit.astype(BF), upper[...])
        last = jnp.where(k == H, 1, 0)
        other_way = last * jnp.where(e % 2 == direction, 0, 1)
        sel = jnp.where(count == slot_row.astype(F32), hit, 0.0)
        sel = jnp.where(other_way == 1, 0.0, sel)
        pick = sel.astype(BF)
        weighted = ((jnp.where(hit0, wts[0], 0.0) + jnp.where(hit1, wts[1], 0.0)) * sel).astype(BF)

        reach = jnp.zeros((1, T), I32)
        for i in range(2):
            dist = ids[i] // PL - s
            dist = jnp.where(dist < 0, dist + NZ, dist)
            odd = ids[i] % 2
            up_way = jnp.where(dist < H, dist, jnp.where((dist == H) & (odd == 0), H, 0))
            down_way = jnp.where(dist > H, NZ - dist, jnp.where((dist == H) & (odd == 1), H, 0))
            reach = jnp.maximum(reach, jnp.where(direction == 0, up_way, down_way))

        def place(kk):
            mask = jnp.where(reach >= kk, 1.0, 0.0)
            pos = mm(jnp.broadcast_to(mask, (8, T)).astype(BF), upper[...])[0:1, :].astype(I32)
            pos = jnp.where(reach >= kk, pos, -1)
            col = lax.broadcasted_iota(I32, (1, T), 1)
            pos = jnp.where(kk >= KP, pos, col)
            return jnp.where(t_row == pos, 1.0, 0.0).astype(BF)

        here, after = place(k), place(k + 1)
        ex[direction, k] = mm_nt(pick, here).astype(BF)
        cm[direction, k] = mm_nt(here, weighted).astype(BF)
        sm[direction, k] = mm_nt(after, here).astype(BF)
        st[direction, k] = mm_nt(here, after).astype(BF)

    def build_steps(lo, hi):
        def one(i, _):
            build(i % 2, lo + i // 2)
            return 0

        lax.fori_loop(0, 2 * (hi - lo), one, 0)

    q_row = (lax.broadcasted_iota(I32, (NR, 1), 0) // CAP) % Q

    def only_q_rows(v, q):
        return jnp.where(q_row == q, v.astype(F32), 0.0).astype(BF)

    q_col = (lax.broadcasted_iota(I32, (1, NR), 1) // CAP) % Q

    def only_q_cols(v, q):
        return jnp.where(q_col == q, v.astype(F32), 0.0).astype(BF)

    def own_block():
        build(0, 0)
        acc[0] = jnp.zeros((NR, DQ), F32)

        def one(q, _):
            acc[0] = acc[0] + mm(only_q_rows(ex[0, 0], q), xs[q])
            return 0

        lax.fori_loop(0, Q, one, 0)
        own = acc[0].astype(BF).reshape(PL, RB, DQ)
        stage[H - 1, :, 1] = own
        rows[H - 1, 0, 1] = own[0]
        plane_start(stage, rows, H + 1, p_send, p_recv)

    def gather(k0):
        for i in range(2):
            k = k0 + i
            plane_wait(stage, rows, k, p_send, p_recv)
            if k == H:
                plane_wait(stage, rows, H + 1, p_send, p_recv)
            got = mm(perm_g[...], rows[k - 1].reshape(PR, DQ)).astype(BF).reshape(Q, SR, DQ)
            xb[:, pl.ds(i * SR, SR), :] = got
        gacc[...] = jnp.zeros_like(gacc)
        uacc[...] = jnp.zeros_like(uacc)

    def piece(i):
        @pl.when(i < Q)
        def _():
            gacc[...] += mm(xb[i], wgv[i])
            uacc[...] += mm(xb[i], wuv[i])

        @pl.when(i == Q)
        def _():
            g = gacc[...]
            hb[...] = ((g / (1.0 + jnp.exp(-g))) * uacc[...]).astype(BF)

        @pl.when(i >= Q)
        def _():
            yb[i - Q] = mm(hb[...], wdv[i - Q]).astype(BF)

    def scatter(k0, then=lambda k: None):
        for i in (1, 0):
            k = k0 + i
            v = yb[:, pl.ds(i * SR, SR), :].reshape(PR, DQ)
            v = mm(perm_s[...], v).astype(BF).reshape(PL, 2, RB, DQ)
            ysend[k - 1] = v
            yrecv[k - 1, 0] = v[0]
            then(k)

    def experts(k0, then=lambda k: None):
        gather(k0)

        def one(i, _):
            piece(i)
            return 0

        lax.fori_loop(0, 2 * Q, one, 0)
        scatter(k0, then)

    def dispatch(k, beside):
        ck = caps[k]
        acc[...] = jnp.zeros_like(acc)

        def chunk(i, _):
            q, direction = i // 2, i % 2
            for at_q in range(Q):
                if relay_at.get((k, at_q), H + 1) <= H:
                    @pl.when(q == at_q)
                    def _():
                        relay_meta(direction, relay_at[k, at_q])
            z_copy(zb.at[direction, k - 1, q, pl.ds(0, ck)], direction, k, q, ck).wait_recv()
            data = zb[direction, k - 1, q, pl.ds(0, ck), :]
            if k < H:
                cn = caps[k + 1]
                if k + 1 >= KP:
                    p = k + 1 - KP
                    zp[direction, p, q, pl.ds(0, cn), :] = mm(sm[direction, k][:cn, :ck], data).astype(BF)
                    source = zp.at[direction, p, q, pl.ds(0, cn)]
                else:
                    source = zb.at[direction, k - 1, q, pl.ds(0, cn)]
                z_copy(source, direction, k + 1, q, cn).start()
            e = only_q_rows(ex[direction, k], q)
            if ck < T:
                e = e[:, :ck]
            block = direction if k < H else 0
            acc[block] = acc[block] + mm(e, data)
            if beside:
                piece(i)
            return 0

        lax.fori_loop(0, 2 * Q, chunk, 0)
        for block in range(2 if k < H else 1):
            v = acc[block].astype(BF).reshape(PL, RB, DQ)
            stage[k - 1, :, block] = v
            rows[k - 1, 0, block] = v[0]
        plane_start(stage, rows, k, p_send, p_recv)

    firsts = list(range(1, H, 2))
    beside = {k0 + 3: k0 for k0 in firsts if k0 + 3 <= H - 2}
    after = [k0 for k0 in firsts if k0 + 3 > H - 2]
    sent = []

    def send_results(k):
        plane_start(ysend, yrecv, k, y_send, y_recv)


    pl.semaphore_wait(barrier, 2 + PL - 1)
    for direction in range(2):
        m_copy(direction, 1).start()
    for q in range(Q):
        for direction in range(2):
            z_copy(xs.at[q], direction, 1, q, caps[1]).start()
    for copy in weight_copies:
        copy.start()
    own_block()
    for direction in range(2):
        relay_meta(direction, 1)
    build_steps(1, 2)
    dispatch(1, False)
    build_steps(2, min(3, H + 1))
    for copy in weight_copies:
        copy.wait()
    builds_after = {2: (3, 4), 3: (4, 5), 4: (5, 7), 5: (7, 8), 7: (8, 9)}
    for k in range(2, H + 1):
        if k in beside:
            gather(beside[k])
        dispatch(k, k in beside)
        if k in beside and k < KP:
            scatter(beside[k], send_results)
            sent.append(beside[k])
        lo, hi = builds_after.get(k, (H + 1, H + 1))
        if lo <= H:
            build_steps(lo, min(hi, H + 1))
    late = [k0 for k0 in beside.values() if k0 not in sent]
    for k0 in late:
        scatter(k0)
    for k0 in after[:-1]:
        experts(k0)
    experts(after[-1], send_results)
    for k0 in list(reversed(after[:-1])) + list(reversed(late)):
        for i in (1, 0):
            send_results(k0 + i)
    send_results(H + 1)

    def r_copy(direction, k, q):
        return pltpu.make_async_remote_copy(
            src_ref=rout.at[direction, k - 1, q, pl.ds(0, caps[k])],
            dst_ref=rin.at[direction, k - 1, q, pl.ds(0, caps[k])],
            send_sem=r_send.at[k - 1], recv_sem=r_recv.at[direction, k - 1, q],
            device_id=backward(direction), device_id_type=MESH,
        )

    for k in range(H, 0, -1):
        ck = caps[k]
        plane_wait(ysend, yrecv, k, y_send, y_recv)

        def back(i, _, k=k, ck=ck):
            q, direction = i // 2, i % 2
            block = direction if k < H else 0
            y = yrecv[k - 1, :, block].reshape(NR, DQ)
            v = mm(only_q_cols(cm[direction, k, pl.ds(0, ck), :], q), y)
            if k < H:
                cn = caps[k + 1]
                r_copy(direction, k + 1, q).wait_recv()
                far = rin[direction, k, q, pl.ds(0, cn), :]
                if k + 1 >= KP:
                    v = v + mm(st[direction, k][:ck, :cn], far)
                else:
                    v = v + far.astype(F32)
            rout[direction, k - 1, q, pl.ds(0, ck), :] = v.astype(BF)
            r_copy(direction, k, q).start()
            return 0

        lax.fori_loop(0, 2 * Q, back, 0)
        plane_sent(stage, rows, k, p_send, p_recv)
        plane_sent(ysend, yrecv, k, y_send, y_recv)
        all_sent(zb.at[:, k - 1, :, pl.ds(0, ck)], z_send.at[k - 1], z_recv.at[0, k - 1, 0])
        if k < H:
            all_sent(rout.at[:, k, :, pl.ds(0, caps[k + 1])], r_send.at[k], r_recv.at[0, k, 0])
    all_sent(metas.at[:, pl.ds(0, H)], m_send.at[0], m_recv.at[0, 1])
    plane_sent(stage, rows, H + 1, p_send, p_recv)
    plane_sent(ysend, yrecv, H + 1, y_send, y_recv)
    plane_wait(ysend, yrecv, H + 1, y_send, y_recv)

    def out_copy(q):
        return pltpu.make_async_copy(out.at[q], out_ref.at[:, pl.ds(q * DQ, DQ)], o_sem.at[q])

    y_own = yrecv[H - 1, :, 1].reshape(NR, DQ)
    for q in range(Q):
        v = mm(only_q_cols(cm[0, 0], q), y_own)
        for direction in range(2):
            r_copy(direction, 1, q).wait_recv()
            v = v + rin[direction, 0, q].astype(F32)
        out[q] = v.astype(BF)
        out_copy(q).start()
    all_sent(rout.at[:, 0, :, pl.ds(0, caps[1])], r_send.at[0], r_recv.at[0, 0, 0])
    for q in range(Q):
        out_copy(q).wait()


def body(hidden_in, expert_ids, route_weights, norm_gain, gate_proj, up_proj, down_proj):
    tokens, width = hidden_in.shape
    chosen = expert_ids.shape[1]
    ep, tp = lax.axis_size("ep"), lax.axis_size("tp")
    fe = gate_proj.shape[2]
    cap = max(2, 2 * chosen * tokens // (ep * tp))
    dm = Dims(ep, tp, tokens, width, fe, cap)
    H, T, DQ, PL, RB, NR, SR = dm.H, dm.T, dm.DQ, dm.PL, dm.RB, dm.NR, dm.SR
    vm = pltpu.VMEM
    packed = max(1, H - dm.KP + 1)
    dma = pltpu.SemaphoreType.DMA
    return pl.pallas_call(
        functools.partial(kernel, dm),
        out_shape=jax.ShapeDtypeStruct((tokens, width), BF),
        in_specs=[pl.BlockSpec(memory_space=pl.ANY)] * 7,
        out_specs=pl.BlockSpec(memory_space=pl.ANY),
        scratch_shapes=[
            vm((tokens, width), BF),
            vm((2, tokens), I32),
            vm((2, tokens), F32),
            vm((1, width), F32),
            vm((Q, T, DQ), BF),
            vm((Q, T, DQ), BF),
            vm((2, H + 1, 4, T), F32),
            vm((2, H, Q, T, DQ), BF),
            vm((2, packed, Q, dm.caps[min(dm.KP, H)], DQ), BF),
            vm((2, H, Q, T, DQ), BF),
            vm((2, H, Q, T, DQ), BF),
            vm((H, PL, 2, RB, DQ), BF),
            vm((H, PL, 2, RB, DQ), BF),
            vm((H, PL, 2, RB, DQ), BF),
            vm((H, PL, 2, RB, DQ), BF),
            vm((2, H + 1, NR, T), BF),
            vm((2, H + 1, T, NR), BF),
            vm((2, H + 1, T, T), BF),
            vm((2, H + 1, T, T), BF),
            vm((NR, T), I32),
            vm((T, T), BF),
            vm((Q * SR, Q * SR), BF),
            vm((Q * SR, Q * SR), BF),
            vm((2, NR, DQ), F32),
            vm((Q, 2 * SR, DQ), BF),
            vm((2 * SR, fe), F32),
            vm((2 * SR, fe), F32),
            vm((2 * SR, fe), BF),
            vm((Q, 2 * SR, DQ), BF),
            vm((Q, DQ, fe), BF),
            vm((Q, DQ, fe), BF),
            vm((Q, fe, DQ), BF),
            dma((7,)),
            dma((Q,)),
            dma((3, Q)),
            dma((1,)),
            dma((2, H + 1)),
            dma((H,)),
            dma((2, H, Q)),
            dma((H + 1,)),
            dma((H + 1,)),
            dma((H + 1,)),
            dma((H + 1,)),
            dma((H,)),
            dma((2, H, Q)),
        ],
        compiler_params=pltpu.CompilerParams(
            collective_id=0, has_side_effects=True, vmem_limit_bytes=66 * 1000 * 1000
        ),
        name="routed_experts",
    )(hidden_in, expert_ids.T, route_weights.T, norm_gain.reshape(1, width), gate_proj, up_proj, down_proj)


def solution(mesh):
    return jax.shard_map(
        body,
        mesh=mesh,
        in_specs=(
            P(("grp", "ep", "tp"), None),
            P(("grp", "ep", "tp"), None),
            P(("grp", "ep", "tp"), None),
            P(),
            P(("ep", "tp"), None, None),
            P(("ep", "tp"), None, None),
            P(("ep", "tp"), None, None),
        ),
        out_specs=P(("grp", "ep", "tp"), None),
        check_vma=False,
    )
```

```python
import functools

import jax
import jax.numpy as jnp
from jax import lax
from jax.experimental import pallas as pl
from jax.experimental.pallas import tpu as pltpu
from jax.sharding import PartitionSpec as P

MESH = pl.DeviceIdType.MESH
BF = jnp.bfloat16
F32 = jnp.float32
I32 = jnp.int32
Q = 4


def mm(a, b):
    return jnp.dot(a, b, preferred_element_type=F32)


def mm_nt(a, b):
    return lax.dot_general(a, b, (((1,), (1,)), ((), ())), preferred_element_type=F32)


class Dims:
    def __init__(self, ep, tp, tokens, width, fe, cap):
        self.NZ, self.NX = ep // 2, tp
        self.T, self.D, self.FE, self.CAP = tokens, width, fe, cap
        self.DQ = width // Q
        self.H = self.NZ // 2
        self.PL = 2 * tp
        self.RB = Q * cap
        self.NR = self.PL * self.RB
        self.SR = self.PL * 2 * cap
        plane = self.PL * cap
        self.caps = [tokens] + [
            min(tokens, (self.H - k) * plane + plane // 2) for k in range(1, self.H + 1)
        ]
        packed = [k for k in range(1, self.H + 1) if self.caps[k] < tokens]
        self.KP = packed[0] if packed else self.H + 1


def kernel(
    dm, hid_in, ids_in, wts_in, gain_in, wg, wu, wd, out_ref,
    hid, idv, wtv, gain, out,
    xs, metas, zb, zp, rin, rout, stage, rows, ysend, yrecv,
    ex, cm, sm, st, e_all, c_all, erow, upper, perm_g, perm_s, acc, xb, gacc, uacc, hb, yb,
    wgv, wuv, wdv,
    i_sem, o_sem, w_sem, m_send, m_recv, z_send, z_recv, p_send, p_recv, y_send, y_recv, r_send, r_recv,
):
    NZ, NX, T, D, FE, CAP = dm.NZ, dm.NX, dm.T, dm.D, dm.FE, dm.CAP
    DQ, H, PL, RB, NR, SR, KP, caps = dm.DQ, dm.H, dm.PL, dm.RB, dm.NR, dm.SR, dm.KP, dm.caps
    ep, x = lax.axis_index("ep"), lax.axis_index("tp")
    z, c = ep // 2, ep % 2

    def at_z(other):
        return {"ep": other * 2 + c, "tp": x}

    def onward(direction):
        return at_z((z + 1 - 2 * direction + NZ) % NZ)

    def backward(direction):
        return at_z((z - 1 + 2 * direction + NZ) % NZ)

    def in_plane(j):
        dc, dx = j // NX, j % NX
        return {"ep": z * 2 + (c + dc) % 2, "tp": (x + dx) % NX}

    def mirror(j):
        return (j // NX) * NX + (NX - j % NX) % NX

    barrier = pltpu.get_barrier_semaphore()
    for direction in range(2):
        pl.semaphore_signal(barrier, inc=1, device_id=onward(direction), device_id_type=MESH)
    for j in range(1, PL):
        pl.semaphore_signal(barrier, inc=1, device_id=in_plane(j), device_id_type=MESH)

    small_copies = [
        pltpu.make_async_copy(ids_in, idv, i_sem.at[0]),
        pltpu.make_async_copy(wts_in, wtv, i_sem.at[1]),
        pltpu.make_async_copy(gain_in, gain, i_sem.at[2]),
    ]
    part = T // 4
    hid_copies = [
        pltpu.make_async_copy(hid_in.at[pl.ds(i * part, part)], hid.at[pl.ds(i * part, part)], i_sem.at[3 + i])
        for i in range(4)
    ]
    for copy in [small_copies[2]] + hid_copies + small_copies[:2]:
        copy.start()
    weight_copies = []
    for q in range(Q):
        weight_copies.append(pltpu.make_async_copy(wg.at[0, pl.ds(q * DQ, DQ)], wgv.at[q], w_sem.at[0, q]))
        weight_copies.append(pltpu.make_async_copy(wu.at[0, pl.ds(q * DQ, DQ)], wuv.at[q], w_sem.at[1, q]))
        weight_copies.append(pltpu.make_async_copy(wd.at[0, :, pl.ds(q * DQ, DQ)], wdv.at[q], w_sem.at[2, q]))
    r_id = lax.broadcasted_iota(I32, (NR, T), 0)
    j_id = r_id // RB
    dx_id, dc_id = j_id % NX, j_id // NX
    erow[...] = z * PL + ((c + dc_id) % 2) * NX + (x + dx_id) % NX
    slot_row = lax.broadcasted_iota(I32, (NR, T), 0) % CAP
    t_row = lax.broadcasted_iota(I32, (T, T), 0)
    t_col = lax.broadcasted_iota(I32, (T, T), 1)
    upper[...] = jnp.where(t_row < t_col, 1.0, 0.0).astype(BF)
    PR = Q * SR
    a_id = lax.broadcasted_iota(I32, (PR, PR), 0)
    n_id = lax.broadcasted_iota(I32, (PR, PR), 1)
    q_of, m_of = a_id // SR, a_id % SR
    perm_g[...] = jnp.where(n_id == (m_of // CAP) * RB + q_of * CAP + m_of % CAP, 1.0, 0.0).astype(BF)
    q_of, m_of = n_id // SR, n_id % SR
    perm_s[...] = jnp.where(a_id == (m_of // CAP) * RB + q_of * CAP + m_of % CAP, 1.0, 0.0).astype(BF)

    small_copies[2].wait()
    NB = min(16, part)

    def norm_rows(b, _):
        r = pl.ds(pl.multiple_of(b * NB, NB), NB)
        v = hid[r, :].astype(F32)
        scale = lax.rsqrt(jnp.mean(v * v, axis=-1, keepdims=True) + 1e-06)
        n = ((v * scale) * gain[...]).astype(BF)
        for q in range(Q):
            xs[q, r, :] = n[:, q * DQ:(q + 1) * DQ]
        return 0

    for i in range(4):
        hid_copies[i].wait()
        lax.fori_loop(i * (part // NB), (i + 1) * (part // NB), norm_rows, 0)

    small_copies[0].wait()
    small_copies[1].wait()
    for direction in range(2):
        metas[direction, 0, 0:2, :] = idv[...].astype(F32)
        metas[direction, 0, 2:4, :] = wtv[...]

    def z_copy(src, direction, k, q, rows_sent):
        return pltpu.make_async_remote_copy(
            src_ref=src, dst_ref=zb.at[direction, k - 1, q, pl.ds(0, rows_sent)],
            send_sem=z_send.at[k - 1], recv_sem=z_recv.at[direction, k - 1, q],
            device_id=onward(direction), device_id_type=MESH,
        )

    def m_copy(direction, k):
        return pltpu.make_async_remote_copy(
            src_ref=metas.at[direction, k - 1], dst_ref=metas.at[direction, k],
            send_sem=m_send.at[0], recv_sem=m_recv.at[direction, k],
            device_id=onward(direction), device_id_type=MESH,
        )

    def relay_meta(direction, k):
        m_copy(direction, k).wait_recv()
        if k < H:
            m_copy(direction, k + 1).start()

    relay_at = {(1, 3): 2, (2, 2): 3, (3, 1): 4, (4, 0): 5, (4, 3): 6, (5, 2): 7, (6, 1): 8}
    assert H <= 8

    def blocks(ref, t, j):
        return ref.at[t - 1, j] if t < H else ref.at[H - 1, j, t - H]

    def plane_copy(src, dst, t, j, to, send, recv):
        return pltpu.make_async_remote_copy(
            src_ref=blocks(src, t, j), dst_ref=blocks(dst, t, to), send_sem=send.at[t - 1], recv_sem=recv.at[t - 1],
            device_id=in_plane(1 if j is others else j), device_id_type=MESH,
        )

    others = pl.ds(1, PL - 1)

    peers = sorted(range(1, PL), key=lambda j: -min(j % NX, NX - j % NX))

    def plane_start(src, dst, t, send, recv):
        for j in peers:
            plane_copy(src, dst, t, j, mirror(j), send, recv).start()

    def plane_wait(src, dst, t, send, recv):
        plane_copy(src, dst, t, others, others, send, recv).wait_recv()

    def plane_sent(src, dst, t, send, recv):
        plane_copy(src, dst, t, others, others, send, recv).wait_send()

    def all_sent(src, send, recv):
        pltpu.make_async_remote_copy(
            src_ref=src, dst_ref=src, send_sem=send, recv_sem=recv, device_id=onward(0), device_id_type=MESH
        ).wait_send()

    def build(direction, k):
        s = (z + NZ - k + 2 * k * direction) % NZ
        m = metas[direction, k]
        ids = [m[i:i + 1, :].astype(I32) for i in range(2)]
        wts = [m[2 + i:3 + i, :] for i in range(2)]
        e = erow[...]
        hit0, hit1 = e == ids[0], e == ids[1]
        hit = jnp.where(hit0, 1.0, 0.0) + jnp.where(hit1, 1.0, 0.0)
        count = mm(hit.astype(BF), upper[...])
        last = jnp.where(k == H, 1, 0)
        other_way = last * jnp.where(e % 2 == direction, 0, 1)
        sel = jnp.where(count == slot_row.astype(F32), hit, 0.0)
        sel = jnp.where(other_way == 1, 0.0, sel)
        pick = sel.astype(BF)
        weighted = ((jnp.where(hit0, wts[0], 0.0) + jnp.where(hit1, wts[1], 0.0)) * sel).astype(BF)

        reach = jnp.zeros((1, T), I32)
        for i in range(2):
            dist = ids[i] // PL - s
            dist = jnp.where(dist < 0, dist + NZ, dist)
            odd = ids[i] % 2
            up_way = jnp.where(dist < H, dist, jnp.where((dist == H) & (odd == 0), H, 0))
            down_way = jnp.where(dist > H, NZ - dist, jnp.where((dist == H) & (odd == 1), H, 0))
            reach = jnp.maximum(reach, jnp.where(direction == 0, up_way, down_way))

        def place(kk):
            mask = jnp.where(reach >= kk, 1.0, 0.0)
            pos = mm(jnp.broadcast_to(mask, (8, T)).astype(BF), upper[...])[0:1, :].astype(I32)
            pos = jnp.where(reach >= kk, pos, -1)
            col = lax.broadcasted_iota(I32, (1, T), 1)
            pos = jnp.where(kk >= KP, pos, col)
            return jnp.where(t_row == pos, 1.0, 0.0).astype(BF)

        here, after = place(k), place(k + 1)
        ex[direction, k] = mm_nt(pick, here).astype(BF)
        cm[direction, k] = mm_nt(here, weighted).astype(BF)
        sm[direction, k] = mm_nt(after, here).astype(BF)
        st[direction, k] = mm_nt(here, after).astype(BF)

    def build_steps(lo, hi):
        def one(i, _):
            build(i % 2, lo + i // 2)
            return 0

        lax.fori_loop(0, 2 * (hi - lo), one, 0)

    q_row = (lax.broadcasted_iota(I32, (NR, 1), 0) // CAP) % Q

    def only_q_rows(v, q):
        return jnp.where(q_row == q, v.astype(F32), 0.0).astype(BF)

    q_col = (lax.broadcasted_iota(I32, (1, NR), 1) // CAP) % Q

    def only_q_cols(v, q):
        return jnp.where(q_col == q, v.astype(F32), 0.0).astype(BF)

    cH = caps[H]
    n_all = 2 * Q * cH

    def build_last():
        r_ax, n_ax = lax.broadcasted_iota(I32, (T, n_all), 0), lax.broadcasted_iota(I32, (T, n_all), 1)
        e_sum = jnp.zeros((NR, n_all), F32)
        for direction in range(2):
            spread = jnp.where((n_ax % cH == r_ax) & (n_ax // (Q * cH) == direction), 1.0, 0.0).astype(BF)
            e_sum = e_sum + mm(ex[direction, H], spread)
        q_n = (lax.broadcasted_iota(I32, (1, n_all), 1) // cH) % Q
        e_all[...] = jnp.where(q_row == q_n, e_sum, 0.0).astype(BF)
        n_ax, r_ax = lax.broadcasted_iota(I32, (n_all, T), 0), lax.broadcasted_iota(I32, (n_all, T), 1)
        c_sum = jnp.zeros((n_all, NR), F32)
        for direction in range(2):
            spread = jnp.where((n_ax % cH == r_ax) & (n_ax // (Q * cH) == direction), 1.0, 0.0).astype(BF)
            c_sum = c_sum + mm(spread, cm[direction, H])
        q_n = (lax.broadcasted_iota(I32, (n_all, 1), 0) // cH) % Q
        c_all[...] = jnp.where(q_n == q_col, c_sum, 0.0).astype(BF)

    def own_block():
        build(0, 0)
        acc[0] = jnp.zeros((NR, DQ), F32)

        def one(q, _):
            acc[0] = acc[0] + mm(only_q_rows(ex[0, 0], q), xs[q])
            return 0

        lax.fori_loop(0, Q, one, 0)
        own = acc[0].astype(BF).reshape(PL, RB, DQ)
        stage[H - 1, :, 1] = own
        rows[H - 1, 0, 1] = own[0]
        plane_start(stage, rows, H + 1, p_send, p_recv)

    def gather(k0):
        for i in range(2):
            k = k0 + i
            plane_wait(stage, rows, k, p_send, p_recv)
            if k == H:
                plane_wait(stage, rows, H + 1, p_send, p_recv)
            got = mm(perm_g[...], rows[k - 1].reshape(PR, DQ)).astype(BF).reshape(Q, SR, DQ)
            xb[:, pl.ds(i * SR, SR), :] = got
        gacc[...] = jnp.zeros_like(gacc)
        uacc[...] = jnp.zeros_like(uacc)

    def piece(i):
        @pl.when(i < Q)
        def _():
            gacc[...] += mm(xb[i], wgv[i])
            uacc[...] += mm(xb[i], wuv[i])

        @pl.when(i == Q)
        def _():
            g = gacc[...]
            hb[...] = ((g / (1.0 + jnp.exp(-g))) * uacc[...]).astype(BF)

        @pl.when(i >= Q)
        def _():
            yb[i - Q] = mm(hb[...], wdv[i - Q]).astype(BF)

    def scatter(k0, then=lambda k: None):
        for i in (1, 0):
            k = k0 + i
            v = yb[:, pl.ds(i * SR, SR), :].reshape(PR, DQ)
            v = mm(perm_s[...], v).astype(BF).reshape(PL, 2, RB, DQ)
            ysend[k - 1] = v
            yrecv[k - 1, 0] = v[0]
            then(k)

    def experts(k0, then=lambda k: None):
        gather(k0)

        def one(i, _):
            piece(i)
            return 0

        lax.fori_loop(0, 2 * Q, one, 0)
        scatter(k0, then)

    def dispatch_last():
        def arrived(i, _):
            q, direction = i // 2, i % 2
            z_copy(zb.at[direction, H - 1, q, pl.ds(0, cH)], direction, H, q, cH).wait_recv()
            return 0

        lax.fori_loop(0, 2 * Q, arrived, 0)
        data = zb[:, H - 1, :, pl.ds(0, cH), :].reshape(n_all, DQ)
        v = mm(e_all[...], data).astype(BF).reshape(PL, RB, DQ)
        stage[H - 1, :, 0] = v
        rows[H - 1, 0, 0] = v[0]
        plane_start(stage, rows, H, p_send, p_recv)

    def dispatch(k, beside):
        ck = caps[k]
        acc[...] = jnp.zeros_like(acc)

        def chunk(i, _):
            q, direction = i // 2, i % 2
            for at_q in range(Q):
                if relay_at.get((k, at_q), H + 1) <= H:
                    @pl.when(q == at_q)
                    def _():
                        relay_meta(direction, relay_at[k, at_q])
            z_copy(zb.at[direction, k - 1, q, pl.ds(0, ck)], direction, k, q, ck).wait_recv()
            data = zb[direction, k - 1, q, pl.ds(0, ck), :]
            cn = caps[k + 1]
            if k + 1 >= KP:
                p = k + 1 - KP
                zp[direction, p, q, pl.ds(0, cn), :] = mm(sm[direction, k][:cn, :ck], data).astype(BF)
                source = zp.at[direction, p, q, pl.ds(0, cn)]
            else:
                source = zb.at[direction, k - 1, q, pl.ds(0, cn)]
            z_copy(source, direction, k + 1, q, cn).start()
            e = only_q_rows(ex[direction, k], q)
            if ck < T:
                e = e[:, :ck]
            acc[direction] = acc[direction] + mm(e, data)
            if beside:
                piece(i)
            return 0

        lax.fori_loop(0, 2 * Q, chunk, 0)
        for block in range(2):
            v = acc[block].astype(BF).reshape(PL, RB, DQ)
            stage[k - 1, :, block] = v
            rows[k - 1, 0, block] = v[0]
        plane_start(stage, rows, k, p_send, p_recv)

    firsts = list(range(1, H, 2))
    beside = {k0 + 3: k0 for k0 in firsts if k0 + 3 <= H - 2}
    after = [k0 for k0 in firsts if k0 + 3 > H - 2]
    sent = []

    def send_results(k):
        plane_start(ysend, yrecv, k, y_send, y_recv)


    pl.semaphore_wait(barrier, 2 + PL - 1)
    for direction in range(2):
        m_copy(direction, 1).start()
    for q in range(Q):
        for direction in range(2):
            z_copy(xs.at[q], direction, 1, q, caps[1]).start()
    for copy in weight_copies:
        copy.start()
    own_block()
    for direction in range(2):
        relay_meta(direction, 1)
    build_steps(1, 2)
    dispatch(1, False)
    build_steps(2, min(3, H + 1))
    if H == 2:
        build_last()
    for copy in weight_copies:
        copy.wait()
    builds_after = {2: (3, 4), 3: (4, 5), 4: (5, 7), 5: (7, 8), 7: (8, 9)}
    for k in range(2, H + 1):
        if k in beside:
            gather(beside[k])
        if k == H:
            dispatch_last()
        else:
            dispatch(k, k in beside)
        if k in beside and k < KP:
            scatter(beside[k], send_results)
            sent.append(beside[k])
        lo, hi = builds_after.get(k, (H + 1, H + 1))
        if lo <= H:
            build_steps(lo, min(hi, H + 1))
            if lo <= H < hi:
                build_last()
    late = [k0 for k0 in beside.values() if k0 not in sent]
    for k0 in late:
        scatter(k0)
    for k0 in after[:-1]:
        experts(k0)
    experts(after[-1], send_results)
    for k0 in list(reversed(after[:-1])) + list(reversed(late)):
        for i in (1, 0):
            send_results(k0 + i)
    send_results(H + 1)

    def r_copy(direction, k, q):
        return pltpu.make_async_remote_copy(
            src_ref=rout.at[direction, k - 1, q, pl.ds(0, caps[k])],
            dst_ref=rin.at[direction, k - 1, q, pl.ds(0, caps[k])],
            send_sem=r_send.at[k - 1], recv_sem=r_recv.at[direction, k - 1, q],
            device_id=backward(direction), device_id_type=MESH,
        )

    for k in range(H, 0, -1):
        ck = caps[k]
        plane_wait(ysend, yrecv, k, y_send, y_recv)

        if k == H:
            v = mm(c_all[...], yrecv[H - 1, :, 0].reshape(NR, DQ)).astype(BF)
            rout[:, H - 1, :, pl.ds(0, cH), :] = v.reshape(2, Q, cH, DQ)

        def back(i, _, k=k, ck=ck):
            q, direction = i // 2, i % 2
            if k < H:
                y = yrecv[k - 1, :, direction].reshape(NR, DQ)
                v = mm(only_q_cols(cm[direction, k, pl.ds(0, ck), :], q), y)
                cn = caps[k + 1]
                r_copy(direction, k + 1, q).wait_recv()
                far = rin[direction, k, q, pl.ds(0, cn), :]
                if k + 1 >= KP:
                    v = v + mm(st[direction, k][:ck, :cn], far)
                else:
                    v = v + far.astype(F32)
                rout[direction, k - 1, q, pl.ds(0, ck), :] = v.astype(BF)
            r_copy(direction, k, q).start()
            return 0

        lax.fori_loop(0, 2 * Q, back, 0)
        plane_sent(stage, rows, k, p_send, p_recv)
        plane_sent(ysend, yrecv, k, y_send, y_recv)
        all_sent(zb.at[:, k - 1, :, pl.ds(0, ck)], z_send.at[k - 1], z_recv.at[0, k - 1, 0])
        if k < H:
            all_sent(rout.at[:, k, :, pl.ds(0, caps[k + 1])], r_send.at[k], r_recv.at[0, k, 0])
    all_sent(metas.at[:, pl.ds(0, H)], m_send.at[0], m_recv.at[0, 1])
    plane_sent(stage, rows, H + 1, p_send, p_recv)
    plane_sent(ysend, yrecv, H + 1, y_send, y_recv)
    plane_wait(ysend, yrecv, H + 1, y_send, y_recv)

    def out_copy(q):
        return pltpu.make_async_copy(out.at[q], out_ref.at[:, pl.ds(q * DQ, DQ)], o_sem.at[q])

    y_own = yrecv[H - 1, :, 1].reshape(NR, DQ)
    for q in range(Q):
        v = mm(only_q_cols(cm[0, 0], q), y_own)
        for direction in range(2):
            r_copy(direction, 1, q).wait_recv()
            v = v + rin[direction, 0, q].astype(F32)
        out[q] = v.astype(BF)
        out_copy(q).start()
    all_sent(rout.at[:, 0, :, pl.ds(0, caps[1])], r_send.at[0], r_recv.at[0, 0, 0])
    for q in range(Q):
        out_copy(q).wait()


def body(hidden_in, expert_ids, route_weights, norm_gain, gate_proj, up_proj, down_proj):
    tokens, width = hidden_in.shape
    chosen = expert_ids.shape[1]
    ep, tp = lax.axis_size("ep"), lax.axis_size("tp")
    fe = gate_proj.shape[2]
    cap = max(2, 2 * chosen * tokens // (ep * tp))
    dm = Dims(ep, tp, tokens, width, fe, cap)
    H, T, DQ, PL, RB, NR, SR = dm.H, dm.T, dm.DQ, dm.PL, dm.RB, dm.NR, dm.SR
    vm = pltpu.VMEM
    packed = max(1, H - dm.KP + 1)
    dma = pltpu.SemaphoreType.DMA
    return pl.pallas_call(
        functools.partial(kernel, dm),
        out_shape=jax.ShapeDtypeStruct((tokens, width), BF),
        in_specs=[pl.BlockSpec(memory_space=pl.ANY)] * 7,
        out_specs=pl.BlockSpec(memory_space=pl.ANY),
        scratch_shapes=[
            vm((tokens, width), BF),
            vm((2, tokens), I32),
            vm((2, tokens), F32),
            vm((1, width), F32),
            vm((Q, T, DQ), BF),
            vm((Q, T, DQ), BF),
            vm((2, H + 1, 4, T), F32),
            vm((2, H, Q, T, DQ), BF),
            vm((2, packed, Q, dm.caps[min(dm.KP, H)], DQ), BF),
            vm((2, H, Q, T, DQ), BF),
            vm((2, H, Q, T, DQ), BF),
            vm((H, PL, 2, RB, DQ), BF),
            vm((H, PL, 2, RB, DQ), BF),
            vm((H, PL, 2, RB, DQ), BF),
            vm((H, PL, 2, RB, DQ), BF),
            vm((2, H + 1, NR, T), BF),
            vm((2, H + 1, T, NR), BF),
            vm((2, H + 1, T, T), BF),
            vm((2, H + 1, T, T), BF),
            vm((NR, 2 * Q * dm.caps[H]), BF),
            vm((2 * Q * dm.caps[H], NR), BF),
            vm((NR, T), I32),
            vm((T, T), BF),
            vm((Q * SR, Q * SR), BF),
            vm((Q * SR, Q * SR), BF),
            vm((2, NR, DQ), F32),
            vm((Q, 2 * SR, DQ), BF),
            vm((2 * SR, fe), F32),
            vm((2 * SR, fe), F32),
            vm((2 * SR, fe), BF),
            vm((Q, 2 * SR, DQ), BF),
            vm((Q, DQ, fe), BF),
            vm((Q, DQ, fe), BF),
            vm((Q, fe, DQ), BF),
            dma((7,)),
            dma((Q,)),
            dma((3, Q)),
            dma((1,)),
            dma((2, H + 1)),
            dma((H,)),
            dma((2, H, Q)),
            dma((H + 1,)),
            dma((H + 1,)),
            dma((H + 1,)),
            dma((H + 1,)),
            dma((H,)),
            dma((2, H, Q)),
        ],
        compiler_params=pltpu.CompilerParams(
            collective_id=0, has_side_effects=True, vmem_limit_bytes=66 * 1000 * 1000
        ),
        name="routed_experts",
    )(hidden_in, expert_ids.T, route_weights.T, norm_gain.reshape(1, width), gate_proj, up_proj, down_proj)


def solution(mesh):
    return jax.shard_map(
        body,
        mesh=mesh,
        in_specs=(
            P(("grp", "ep", "tp"), None),
            P(("grp", "ep", "tp"), None),
            P(("grp", "ep", "tp"), None),
            P(),
            P(("ep", "tp"), None, None),
            P(("ep", "tp"), None, None),
            P(("ep", "tp"), None, None),
        ),
        out_specs=P(("grp", "ep", "tp"), None),
        check_vma=False,
    )
```

```python
import functools

import jax
import jax.numpy as jnp
from jax import lax
from jax.experimental import pallas as pl
from jax.experimental.pallas import tpu as pltpu
from jax.sharding import PartitionSpec as P

MESH = pl.DeviceIdType.MESH
BF = jnp.bfloat16
F32 = jnp.float32
I32 = jnp.int32
Q = 4


def mm(a, b):
    return jnp.dot(a, b, preferred_element_type=F32)


def mm_nt(a, b):
    return lax.dot_general(a, b, (((1,), (1,)), ((), ())), preferred_element_type=F32)


class Dims:
    def __init__(self, ep, tp, tokens, width, fe, cap):
        self.NZ, self.NX = ep // 2, tp
        self.T, self.D, self.FE, self.CAP = tokens, width, fe, cap
        self.DQ = width // Q
        self.H = self.NZ // 2
        self.PL = 2 * tp
        self.RB = Q * cap
        self.NR = self.PL * self.RB
        self.SR = self.PL * 2 * cap
        plane = self.PL * cap
        self.caps = [tokens] + [
            min(tokens, (self.H - k) * plane + plane // 2) for k in range(1, self.H + 1)
        ]
        packed = [k for k in range(1, self.H + 1) if self.caps[k] < tokens]
        self.KP = packed[0] if packed else self.H + 1


def kernel(
    dm, hid_in, ids_in, wts_in, gain_in, wg, wu, wd, out_ref,
    hid, idv, wtv, gain, out,
    xs, metas, zb, zp, rin, rout, stage, rows, ysend, yrecv,
    ex, cm, sm, st, e_all, c_all, erow, upper, perm_g, perm_s, acc, xb, gacc, uacc, hb, yb,
    wgv, wuv, wdv,
    i_sem, o_sem, w_sem, m_send, m_recv, z_send, z_recv, p_send, p_recv, y_send, y_recv, r_send, r_recv,
):
    NZ, NX, T, D, FE, CAP = dm.NZ, dm.NX, dm.T, dm.D, dm.FE, dm.CAP
    DQ, H, PL, RB, NR, SR, KP, caps = dm.DQ, dm.H, dm.PL, dm.RB, dm.NR, dm.SR, dm.KP, dm.caps
    ep, x = lax.axis_index("ep"), lax.axis_index("tp")
    z, c = ep // 2, ep % 2

    def at_z(other):
        return {"ep": other * 2 + c, "tp": x}

    def onward(direction):
        return at_z((z + 1 - 2 * direction + NZ) % NZ)

    def backward(direction):
        return at_z((z - 1 + 2 * direction + NZ) % NZ)

    def in_plane(j):
        dc, dx = j // NX, j % NX
        return {"ep": z * 2 + (c + dc) % 2, "tp": (x + dx) % NX}

    def mirror(j):
        return (j // NX) * NX + (NX - j % NX) % NX

    barrier = pltpu.get_barrier_semaphore()
    for direction in range(2):
        pl.semaphore_signal(barrier, inc=1, device_id=onward(direction), device_id_type=MESH)
    for j in range(1, PL):
        pl.semaphore_signal(barrier, inc=1, device_id=in_plane(j), device_id_type=MESH)

    small_copies = [
        pltpu.make_async_copy(ids_in, idv, i_sem.at[0]),
        pltpu.make_async_copy(wts_in, wtv, i_sem.at[1]),
        pltpu.make_async_copy(gain_in, gain, i_sem.at[2]),
    ]
    part = T // 4
    hid_copies = [
        pltpu.make_async_copy(hid_in.at[pl.ds(i * part, part)], hid.at[pl.ds(i * part, part)], i_sem.at[3 + i])
        for i in range(4)
    ]
    for copy in [small_copies[2]] + hid_copies + small_copies[:2]:
        copy.start()
    weight_copies = []
    for q in range(Q):
        weight_copies.append(pltpu.make_async_copy(wg.at[0, pl.ds(q * DQ, DQ)], wgv.at[q], w_sem.at[0, q]))
        weight_copies.append(pltpu.make_async_copy(wu.at[0, pl.ds(q * DQ, DQ)], wuv.at[q], w_sem.at[1, q]))
        weight_copies.append(pltpu.make_async_copy(wd.at[0, :, pl.ds(q * DQ, DQ)], wdv.at[q], w_sem.at[2, q]))
    r_id = lax.broadcasted_iota(I32, (NR, T), 0)
    j_id = r_id // RB
    dx_id, dc_id = j_id % NX, j_id // NX
    erow[...] = z * PL + ((c + dc_id) % 2) * NX + (x + dx_id) % NX
    slot_row = lax.broadcasted_iota(I32, (NR, T), 0) % CAP
    t_row = lax.broadcasted_iota(I32, (T, T), 0)
    t_col = lax.broadcasted_iota(I32, (T, T), 1)
    upper[...] = jnp.where(t_row < t_col, 1.0, 0.0).astype(BF)
    PR = Q * SR
    a_id = lax.broadcasted_iota(I32, (PR, PR), 0)
    n_id = lax.broadcasted_iota(I32, (PR, PR), 1)
    q_of, m_of = a_id // SR, a_id % SR
    perm_g[...] = jnp.where(n_id == (m_of // CAP) * RB + q_of * CAP + m_of % CAP, 1.0, 0.0).astype(BF)
    q_of, m_of = n_id // SR, n_id % SR
    perm_s[...] = jnp.where(a_id == (m_of // CAP) * RB + q_of * CAP + m_of % CAP, 1.0, 0.0).astype(BF)

    small_copies[2].wait()
    NB = min(16, part)

    def norm_rows(b, _):
        r = pl.ds(pl.multiple_of(b * NB, NB), NB)
        v = hid[r, :].astype(F32)
        scale = lax.rsqrt(jnp.mean(v * v, axis=-1, keepdims=True) + 1e-06)
        n = ((v * scale) * gain[...]).astype(BF)
        for q in range(Q):
            xs[q, r, :] = n[:, q * DQ:(q + 1) * DQ]
        return 0

    for i in range(4):
        hid_copies[i].wait()
        lax.fori_loop(i * (part // NB), (i + 1) * (part // NB), norm_rows, 0)

    small_copies[0].wait()
    small_copies[1].wait()
    for direction in range(2):
        metas[direction, 0, 0:2, :] = idv[...].astype(F32)
        metas[direction, 0, 2:4, :] = wtv[...]

    def z_copy(src, direction, k, q, rows_sent):
        return pltpu.make_async_remote_copy(
            src_ref=src, dst_ref=zb.at[direction, k - 1, q, pl.ds(0, rows_sent)],
            send_sem=z_send.at[k - 1], recv_sem=z_recv.at[direction, k - 1, q],
            device_id=onward(direction), device_id_type=MESH,
        )

    def m_copy(direction, k):
        return pltpu.make_async_remote_copy(
            src_ref=metas.at[direction, k - 1], dst_ref=metas.at[direction, k],
            send_sem=m_send.at[0], recv_sem=m_recv.at[direction, k],
            device_id=onward(direction), device_id_type=MESH,
        )

    def relay_meta(direction, k):
        m_copy(direction, k).wait_recv()
        if k < H:
            m_copy(direction, k + 1).start()

    relay_at = {(1, 3): 2, (2, 2): 3, (3, 1): 4, (4, 0): 5, (4, 3): 6, (5, 2): 7, (6, 1): 8}
    assert H <= 8

    def blocks(ref, t, j):
        return ref.at[t - 1, j] if t < H else ref.at[H - 1, j, t - H]

    def plane_copy(src, dst, t, j, to, send, recv):
        return pltpu.make_async_remote_copy(
            src_ref=blocks(src, t, j), dst_ref=blocks(dst, t, to), send_sem=send.at[t - 1], recv_sem=recv.at[t - 1],
            device_id=in_plane(1 if j is others else j), device_id_type=MESH,
        )

    others = pl.ds(1, PL - 1)

    def plane_start(src, dst, t, send, recv):
        for j in range(1, PL):
            plane_copy(src, dst, t, j, mirror(j), send, recv).start()

    def plane_wait(src, dst, t, send, recv):
        plane_copy(src, dst, t, others, others, send, recv).wait_recv()

    def plane_sent(src, dst, t, send, recv):
        plane_copy(src, dst, t, others, others, send, recv).wait_send()

    def all_sent(src, send, recv):
        pltpu.make_async_remote_copy(
            src_ref=src, dst_ref=src, send_sem=send, recv_sem=recv, device_id=onward(0), device_id_type=MESH
        ).wait_send()

    def build(direction, k):
        s = (z + NZ - k + 2 * k * direction) % NZ
        m = metas[direction, k]
        ids = [m[i:i + 1, :].astype(I32) for i in range(2)]
        wts = [m[2 + i:3 + i, :] for i in range(2)]
        e = erow[...]
        hit0, hit1 = e == ids[0], e == ids[1]
        hit = jnp.where(hit0, 1.0, 0.0) + jnp.where(hit1, 1.0, 0.0)
        count = mm(hit.astype(BF), upper[...])
        last = jnp.where(k == H, 1, 0)
        other_way = last * jnp.where(e % 2 == direction, 0, 1)
        sel = jnp.where(count == slot_row.astype(F32), hit, 0.0)
        sel = jnp.where(other_way == 1, 0.0, sel)
        pick = sel.astype(BF)
        weighted = ((jnp.where(hit0, wts[0], 0.0) + jnp.where(hit1, wts[1], 0.0)) * sel).astype(BF)

        reach = jnp.zeros((1, T), I32)
        for i in range(2):
            dist = ids[i] // PL - s
            dist = jnp.where(dist < 0, dist + NZ, dist)
            odd = ids[i] % 2
            up_way = jnp.where(dist < H, dist, jnp.where((dist == H) & (odd == 0), H, 0))
            down_way = jnp.where(dist > H, NZ - dist, jnp.where((dist == H) & (odd == 1), H, 0))
            reach = jnp.maximum(reach, jnp.where(direction == 0, up_way, down_way))

        def place(kk):
            mask = jnp.where(reach >= kk, 1.0, 0.0)
            pos = mm(jnp.broadcast_to(mask, (8, T)).astype(BF), upper[...])[0:1, :].astype(I32)
            pos = jnp.where(reach >= kk, pos, -1)
            col = lax.broadcasted_iota(I32, (1, T), 1)
            pos = jnp.where(kk >= KP, pos, col)
            return jnp.where(t_row == pos, 1.0, 0.0).astype(BF)

        here, after = place(k), place(k + 1)
        ex[direction, k] = mm_nt(pick, here).astype(BF)
        cm[direction, k] = mm_nt(here, weighted).astype(BF)
        sm[direction, k] = mm_nt(after, here).astype(BF)
        st[direction, k] = mm_nt(here, after).astype(BF)

    def build_steps(lo, hi):
        def one(i, _):
            build(i % 2, lo + i // 2)
            return 0

        lax.fori_loop(0, 2 * (hi - lo), one, 0)

    q_row = (lax.broadcasted_iota(I32, (NR, 1), 0) // CAP) % Q

    def only_q_rows(v, q):
        return jnp.where(q_row == q, v.astype(F32), 0.0).astype(BF)

    q_col = (lax.broadcasted_iota(I32, (1, NR), 1) // CAP) % Q

    def only_q_cols(v, q):
        return jnp.where(q_col == q, v.astype(F32), 0.0).astype(BF)

    cH = caps[H]
    n_all = 2 * Q * cH

    def build_last():
        r_ax, n_ax = lax.broadcasted_iota(I32, (T, n_all), 0), lax.broadcasted_iota(I32, (T, n_all), 1)
        e_sum = jnp.zeros((NR, n_all), F32)
        for direction in range(2):
            spread = jnp.where((n_ax % cH == r_ax) & (n_ax // (Q * cH) == direction), 1.0, 0.0).astype(BF)
            e_sum = e_sum + mm(ex[direction, H], spread)
        q_n = (lax.broadcasted_iota(I32, (1, n_all), 1) // cH) % Q
        e_all[...] = jnp.where(q_row == q_n, e_sum, 0.0).astype(BF)
        n_ax, r_ax = lax.broadcasted_iota(I32, (n_all, T), 0), lax.broadcasted_iota(I32, (n_all, T), 1)
        c_sum = jnp.zeros((n_all, NR), F32)
        for direction in range(2):
            spread = jnp.where((n_ax % cH == r_ax) & (n_ax // (Q * cH) == direction), 1.0, 0.0).astype(BF)
            c_sum = c_sum + mm(spread, cm[direction, H])
        q_n = (lax.broadcasted_iota(I32, (n_all, 1), 0) // cH) % Q
        c_all[...] = jnp.where(q_n == q_col, c_sum, 0.0).astype(BF)

    def own_block():
        build(0, 0)
        acc[0] = jnp.zeros((NR, DQ), F32)

        def one(q, _):
            acc[0] = acc[0] + mm(only_q_rows(ex[0, 0], q), xs[q])
            return 0

        lax.fori_loop(0, Q, one, 0)
        own = acc[0].astype(BF).reshape(PL, RB, DQ)
        stage[H - 1, :, 1] = own
        rows[H - 1, 0, 1] = own[0]
        plane_start(stage, rows, H + 1, p_send, p_recv)

    def gather(k0):
        for i in range(2):
            k = k0 + i
            plane_wait(stage, rows, k, p_send, p_recv)
            if k == H:
                plane_wait(stage, rows, H + 1, p_send, p_recv)
            got = mm(perm_g[...], rows[k - 1].reshape(PR, DQ)).astype(BF).reshape(Q, SR, DQ)
            xb[:, pl.ds(i * SR, SR), :] = got
        gacc[...] = jnp.zeros_like(gacc)
        uacc[...] = jnp.zeros_like(uacc)

    def piece(i):
        @pl.when(i < Q)
        def _():
            gacc[...] += mm(xb[i], wgv[i])
            uacc[...] += mm(xb[i], wuv[i])

        @pl.when(i == Q)
        def _():
            g = gacc[...]
            hb[...] = ((g / (1.0 + jnp.exp(-g))) * uacc[...]).astype(BF)

        @pl.when(i >= Q)
        def _():
            yb[i - Q] = mm(hb[...], wdv[i - Q]).astype(BF)

    def scatter(k0, then=lambda k: None):
        for i in (1, 0):
            k = k0 + i
            v = yb[:, pl.ds(i * SR, SR), :].reshape(PR, DQ)
            v = mm(perm_s[...], v).astype(BF).reshape(PL, 2, RB, DQ)
            ysend[k - 1] = v
            yrecv[k - 1, 0] = v[0]
            then(k)

    def experts(k0, then=lambda k: None):
        gather(k0)

        def one(i, _):
            piece(i)
            return 0

        lax.fori_loop(0, 2 * Q, one, 0)
        scatter(k0, then)

    def dispatch_last():
        def arrived(i, _):
            q, direction = i // 2, i % 2
            z_copy(zb.at[direction, H - 1, q, pl.ds(0, cH)], direction, H, q, cH).wait_recv()
            return 0

        lax.fori_loop(0, 2 * Q, arrived, 0)
        data = zb[:, H - 1, :, pl.ds(0, cH), :].reshape(n_all, DQ)
        v = mm(e_all[...], data).astype(BF).reshape(PL, RB, DQ)
        stage[H - 1, :, 0] = v
        rows[H - 1, 0, 0] = v[0]
        plane_start(stage, rows, H, p_send, p_recv)

    def dispatch(k, beside):
        ck = caps[k]
        acc[...] = jnp.zeros_like(acc)

        def chunk(i, _):
            q, direction = i // 2, i % 2
            for at_q in range(Q):
                if relay_at.get((k, at_q), H + 1) <= H:
                    @pl.when(q == at_q)
                    def _():
                        relay_meta(direction, relay_at[k, at_q])
            z_copy(zb.at[direction, k - 1, q, pl.ds(0, ck)], direction, k, q, ck).wait_recv()
            data = zb[direction, k - 1, q, pl.ds(0, ck), :]
            cn = caps[k + 1]
            if k + 1 >= KP:
                p = k + 1 - KP
                zp[direction, p, q, pl.ds(0, cn), :] = mm(sm[direction, k][:cn, :ck], data).astype(BF)
                source = zp.at[direction, p, q, pl.ds(0, cn)]
            else:
                source = zb.at[direction, k - 1, q, pl.ds(0, cn)]
            z_copy(source, direction, k + 1, q, cn).start()
            e = only_q_rows(ex[direction, k], q)
            if ck < T:
                e = e[:, :ck]
            acc[direction] = acc[direction] + mm(e, data)
            if beside:
                piece(i)
            return 0

        lax.fori_loop(0, 2 * Q, chunk, 0)
        for block in range(2):
            v = acc[block].astype(BF).reshape(PL, RB, DQ)
            stage[k - 1, :, block] = v
            rows[k - 1, 0, block] = v[0]
        plane_start(stage, rows, k, p_send, p_recv)

    firsts = list(range(1, H, 2))
    beside = {k0 + 3: k0 for k0 in firsts if k0 + 3 <= H - 2}
    after = [k0 for k0 in firsts if k0 + 3 > H - 2]
    sent = []

    def send_results(k):
        plane_start(ysend, yrecv, k, y_send, y_recv)


    pl.semaphore_wait(barrier, 2 + PL - 1)
    for direction in range(2):
        m_copy(direction, 1).start()
    for q in range(Q):
        for direction in range(2):
            z_copy(xs.at[q], direction, 1, q, caps[1]).start()
    for copy in weight_copies:
        copy.start()
    own_block()
    for direction in range(2):
        relay_meta(direction, 1)
    build_steps(1, 2)
    dispatch(1, False)
    build_steps(2, min(3, H + 1))
    if H == 2:
        build_last()
    for copy in weight_copies:
        copy.wait()
    builds_after = {2: (3, 4), 3: (4, 5), 4: (5, 7), 5: (7, 8), 7: (8, 9)}
    for k in range(2, H + 1):
        if k in beside:
            gather(beside[k])
        if k == H:
            dispatch_last()
        else:
            dispatch(k, k in beside)
        if k in beside and k < KP:
            scatter(beside[k], send_results)
            sent.append(beside[k])
        lo, hi = builds_after.get(k, (H + 1, H + 1))
        if lo <= H:
            build_steps(lo, min(hi, H + 1))
            if lo <= H < hi:
                build_last()
    late = [k0 for k0 in beside.values() if k0 not in sent]
    for k0 in late:
        scatter(k0)
    for k0 in after[:-1]:
        experts(k0)
    experts(after[-1], send_results)
    for k0 in list(reversed(after[:-1])) + list(reversed(late)):
        for i in (1, 0):
            send_results(k0 + i)
    send_results(H + 1)

    def r_copy(direction, k, q):
        return pltpu.make_async_remote_copy(
            src_ref=rout.at[direction, k - 1, q, pl.ds(0, caps[k])],
            dst_ref=rin.at[direction, k - 1, q, pl.ds(0, caps[k])],
            send_sem=r_send.at[k - 1],
            recv_sem=z_recv.at[direction, k - 1, q] if k < H else r_recv.at[direction, q],
            device_id=backward(direction), device_id_type=MESH,
        )

    for k in range(H, 0, -1):
        ck = caps[k]
        plane_wait(ysend, yrecv, k, y_send, y_recv)

        if k == H:
            v = mm(c_all[...], yrecv[H - 1, :, 0].reshape(NR, DQ)).astype(BF)
            rout[:, H - 1, :, pl.ds(0, cH), :] = v.reshape(2, Q, cH, DQ)

        def back(i, _, k=k, ck=ck):
            q, direction = i // 2, i % 2
            if k < H:
                y = yrecv[k - 1, :, direction].reshape(NR, DQ)
                v = mm(only_q_cols(cm[direction, k, pl.ds(0, ck), :], q), y)
                cn = caps[k + 1]
                r_copy(direction, k + 1, q).wait_recv()
                far = rin[direction, k, q, pl.ds(0, cn), :]
                if k + 1 >= KP:
                    v = v + mm(st[direction, k][:ck, :cn], far)
                else:
                    v = v + far.astype(F32)
                rout[direction, k - 1, q, pl.ds(0, ck), :] = v.astype(BF)
            r_copy(direction, k, q).start()
            return 0

        lax.fori_loop(0, 2 * Q, back, 0)
        plane_sent(stage, rows, k, p_send, p_recv)
        plane_sent(ysend, yrecv, k, y_send, y_recv)
        all_sent(zb.at[:, k - 1, :, pl.ds(0, ck)], z_send.at[k - 1], z_recv.at[0, k - 1, 0])
        if k < H:
            all_sent(rout.at[:, k, :, pl.ds(0, caps[k + 1])], r_send.at[k], r_recv.at[0, 0])
    all_sent(metas.at[:, pl.ds(0, H)], m_send.at[0], m_recv.at[0, 1])
    plane_sent(stage, rows, H + 1, p_send, p_recv)
    plane_sent(ysend, yrecv, H + 1, y_send, y_recv)
    plane_wait(ysend, yrecv, H + 1, y_send, y_recv)

    def out_copy(q):
        return pltpu.make_async_copy(out.at[q], out_ref.at[:, pl.ds(q * DQ, DQ)], o_sem.at[q])

    y_own = yrecv[H - 1, :, 1].reshape(NR, DQ)
    for q in range(Q):
        v = mm(only_q_cols(cm[0, 0], q), y_own)
        for direction in range(2):
            r_copy(direction, 1, q).wait_recv()
            v = v + rin[direction, 0, q].astype(F32)
        out[q] = v.astype(BF)
        out_copy(q).start()
    all_sent(rout.at[:, 0, :, pl.ds(0, caps[1])], r_send.at[0], r_recv.at[0, 0])
    for q in range(Q):
        out_copy(q).wait()


def body(hidden_in, expert_ids, route_weights, norm_gain, gate_proj, up_proj, down_proj):
    tokens, width = hidden_in.shape
    chosen = expert_ids.shape[1]
    ep, tp = lax.axis_size("ep"), lax.axis_size("tp")
    fe = gate_proj.shape[2]
    cap = max(2, 2 * chosen * tokens // (ep * tp))
    dm = Dims(ep, tp, tokens, width, fe, cap)
    H, T, DQ, PL, RB, NR, SR = dm.H, dm.T, dm.DQ, dm.PL, dm.RB, dm.NR, dm.SR
    vm = pltpu.VMEM
    packed = max(1, H - dm.KP + 1)
    dma = pltpu.SemaphoreType.DMA
    return pl.pallas_call(
        functools.partial(kernel, dm),
        out_shape=jax.ShapeDtypeStruct((tokens, width), BF),
        in_specs=[pl.BlockSpec(memory_space=pl.ANY)] * 7,
        out_specs=pl.BlockSpec(memory_space=pl.ANY),
        scratch_shapes=[
            vm((tokens, width), BF),
            vm((2, tokens), I32),
            vm((2, tokens), F32),
            vm((1, width), F32),
            vm((Q, T, DQ), BF),
            vm((Q, T, DQ), BF),
            vm((2, H + 1, 4, T), F32),
            vm((2, H, Q, T, DQ), BF),
            vm((2, packed, Q, dm.caps[min(dm.KP, H)], DQ), BF),
            vm((2, H, Q, T, DQ), BF),
            vm((2, H, Q, T, DQ), BF),
            vm((H, PL, 2, RB, DQ), BF),
            vm((H, PL, 2, RB, DQ), BF),
            vm((H, PL, 2, RB, DQ), BF),
            vm((H, PL, 2, RB, DQ), BF),
            vm((2, H + 1, NR, T), BF),
            vm((2, H + 1, T, NR), BF),
            vm((2, H + 1, T, T), BF),
            vm((2, H + 1, T, T), BF),
            vm((NR, 2 * Q * dm.caps[H]), BF),
            vm((2 * Q * dm.caps[H], NR), BF),
            vm((NR, T), I32),
            vm((T, T), BF),
            vm((Q * SR, Q * SR), BF),
            vm((Q * SR, Q * SR), BF),
            vm((2, NR, DQ), F32),
            vm((Q, 2 * SR, DQ), BF),
            vm((2 * SR, fe), F32),
            vm((2 * SR, fe), F32),
            vm((2 * SR, fe), BF),
            vm((Q, 2 * SR, DQ), BF),
            vm((Q, DQ, fe), BF),
            vm((Q, DQ, fe), BF),
            vm((Q, fe, DQ), BF),
            dma((7,)),
            dma((Q,)),
            dma((3, Q)),
            dma((1,)),
            dma((2, H + 1)),
            dma((H,)),
            dma((2, H, Q)),
            dma((H + 1,)),
            dma((H + 1,)),
            dma((H + 1,)),
            dma((H + 1,)),
            dma((H,)),
            dma((2, Q)),
        ],
        compiler_params=pltpu.CompilerParams(
            collective_id=0, has_side_effects=True, vmem_limit_bytes=66 * 1000 * 1000
        ),
        name="routed_experts",
    )(hidden_in, expert_ids.T, route_weights.T, norm_gain.reshape(1, width), gate_proj, up_proj, down_proj)


def solution(mesh):
    return jax.shard_map(
        body,
        mesh=mesh,
        in_specs=(
            P(("grp", "ep", "tp"), None),
            P(("grp", "ep", "tp"), None),
            P(("grp", "ep", "tp"), None),
            P(),
            P(("ep", "tp"), None, None),
            P(("ep", "tp"), None, None),
            P(("ep", "tp"), None, None),
        ),
        out_specs=P(("grp", "ep", "tp"), None),
        check_vma=False,
    )
```
